512 devices in a mesh: sp: 32 (over z, x), tp: 16 (over y, core).
Axes of the slice: x: 4, y: 8, z: 8, core: 2. Of those that a mesh axis runs over, the one named last changes fastest.
Arguments:
- resid: bfloat16 [4096, 2048], P('sp'), may hold values from -6 to 6
- norm_gain: float32 [2048], replicated, may hold values from 0.1 to 1.9
- cotangent: bfloat16 [4096, 2048], P('sp'), may hold values from -6 to 6
- route_ids: int32 [4096, 2], P('sp'), may hold values from 0 to 31, all different within a row; in each aligned block of 128 rows (0 to 127, 128 to 255, ...) at most 12 rows name the same one
- route_weight: float32 [4096, 2], P('sp'), may hold values from 0.25 to 2.25
- expert_gate: bfloat16 [32, 2048, 2048], P('sp', None, 'tp'), may hold values from -0.125 to 0.125
- expert_up: bfloat16 [32, 2048, 2048], P('sp', None, 'tp'), may hold values from -0.125 to 0.125
- expert_down: bfloat16 [32, 2048, 2048], P('sp', 'tp'), may hold values from -0.125 to 0.125
- out_proj: bfloat16 [2048, 4096], P('sp', 'tp'), may hold values from -0.09375 to 0.09375
- mixed: bfloat16 [4096, 4096], P('sp', 'tp'), may hold values from -6 to 6
- query: bfloat16 [4096, 2048], P('sp', 'tp'), may hold values from -6 to 6
- key: bfloat16 [4096, 2048], P('sp', 'tp'), may hold values from -1.5 to 1.5
- value: bfloat16 [4096, 4096], P('sp', 'tp'), may hold values from -6 to 6
- log_decay: float32 [4096, 2048], P('sp', 'tp'), may hold values from -1 to 0, as said below
- span_state: float32 [32, 16, 128, 256], P('sp', 'tp'), may hold values from -24 to 24
Outputs:
- grad_expert_gate: bfloat16 [32, 2048, 2048], P('sp', None, 'tp')
- grad_expert_up: bfloat16 [32, 2048, 2048], P('sp', None, 'tp')
- grad_expert_down: bfloat16 [32, 2048, 2048], P('sp', 'tp')
- grad_out_proj: float32 [2048, 4096], P('sp', 'tp')
- grad_query: bfloat16 [4096, 2048], P('sp', 'tp')
- grad_key: bfloat16 [4096, 2048], P('sp', 'tp')
- grad_value: bfloat16 [4096, 4096], P('sp', 'tp')
- grad_log_decay: float32 [4096, 2048], P('sp', 'tp')
The draws below stay inside these ranges and needn't reach their ends.
Inputs may be any that keep to these rules, and one draw needn't show every extreme that they name: `route_ids`: A row names 2 different experts. Within each aligned block of 128 rows (the rows of one index of sp) no expert is named by more than 12 rows, and in every draw some expert is named by exactly 12 rows of some block. `log_decay`: every entry is zero or negative.
All inputs are finite; a program needn't handle non-finite values.
Results may differ from the reference program's by a relative error of at most 0.023.
Values may be sent and summed in bfloat16 or wider, within the bound.
No kernel may reach another device: no remote copies, remote signals or barrier semaphores. Data moves between devices by JAX's collectives and lax.ppermute only.
A program may use at most 64 MiB of HBM per device.

```python
import math
import jax
import jax.numpy as jnp
import numpy as np
from jax import lax

D = 2048
ATTENTION_HEADS = 16
KEY_CHANNELS = 128
DV = 256
FE = 2048
TOP = 2
BLOCK = 64
TOK_DEV = 128
EXPERTS = 32
TOKEN_POSITIONS = 4096
CAP = 12
SPANS = 32
N_SP = 32
N_TP = 16


def draw_log_decay(key, part):
    random_keys = jax.random.split(jax.random.fold_in(key, 17), 8)
    fast_share = 0.5
    slow_base = jnp.exp(jax.random.uniform(random_keys[1], (ATTENTION_HEADS, KEY_CHANNELS), jnp.float32, jnp.log(0.1), jnp.log(0.6))) / TOKEN_POSITIONS
    fast_base = jnp.exp(jax.random.uniform(random_keys[2], (ATTENTION_HEADS, KEY_CHANNELS), jnp.float32, jnp.log(1.0 / 80.0), jnp.log(1.0 / 40.0)))
    fast_heads = jax.random.bernoulli(random_keys[0], fast_share, (ATTENTION_HEADS,))
    base_rate = jnp.where(fast_heads[:, None], fast_base, slow_base)
    span_factor = jnp.exp(jax.random.uniform(random_keys[3], (TOKEN_POSITIONS // TOK_DEV, 1, 1), jnp.float32, jnp.log(0.5), jnp.log(2.0)))
    span_factor = jnp.repeat(span_factor, TOK_DEV, axis=0)
    position_factor = jax.random.uniform(random_keys[4], (TOKEN_POSITIONS, ATTENTION_HEADS, KEY_CHANNELS), jnp.float32, 0.5, 1.5)
    decay_speeds = base_rate[None, :, :] * span_factor * position_factor
    cluster_start = jax.random.randint(random_keys[5], (ATTENTION_HEADS, 1), 0, TOKEN_POSITIONS)
    cluster_spacing = jax.random.randint(random_keys[7], (ATTENTION_HEADS, 1), 1, TOKEN_POSITIONS)
    cluster_location = jnp.concatenate([cluster_start, (cluster_start + cluster_spacing) % TOKEN_POSITIONS], axis=1)
    cluster_length = jax.random.uniform(random_keys[6], (ATTENTION_HEADS, 2), jnp.float32, 0.22, 0.69)
    token_places = jnp.arange(TOKEN_POSITIONS, dtype=jnp.int32)[:, None, None]
    cluster_count = jnp.sum(jnp.where(token_places == cluster_location[None, :, :], cluster_length[None, :, :], 0.0), axis=2)
    return (-(decay_speeds + cluster_count[:, :, None])).reshape(TOKEN_POSITIONS, ATTENTION_HEADS * KEY_CHANNELS).astype(jnp.float32)


def spiked(entries, key, source, target, blocks, factor):
    def block_of(dim):
        return (jnp.arange(entries.shape[dim]) // (entries.shape[dim] // blocks)).reshape((-1,) + (1,) * (entries.ndim - 1 - dim))

    one_side = jax.random.permutation(key, blocks)[block_of(target)]
    other_side = (block_of(target) + blocks // 2) % blocks
    return jnp.where((block_of(source) == one_side) | (block_of(source) == other_side), factor * entries, entries)


def levels(key, dims, cuts, least, top_value):
    level = 1.0
    for dim, shards_of in cuts:
        heights = jax.random.uniform(jax.random.fold_in(jax.random.fold_in(key, 6), dim), (shards_of,), jnp.float32, least / len(cuts), top_value / len(cuts))
        level = level * jnp.repeat(jnp.exp(heights), dims[dim] // shards_of).reshape((-1,) + (1,) * (len(dims) - 1 - dim))
    return level


def shared_out(key, own, number, rows, count, top, limit, slope):
    order = jax.random.permutation(key, count)
    packed, ordinary = portions_of(count, rows * top, limit, slope, True), portions_of(count, rows * top, limit, slope, False)
    places = jnp.arange(count)

    def named(tallies, turn):
        used = int((tallies > 0).sum())
        fixed = max(1, used // 4)
        moved = fixed + (places - fixed + turn * (used - fixed)) % max(1, count - fixed)
        return jnp.zeros((count,), jnp.int32).at[order[jnp.where(places < fixed, places, moved)]].set(jnp.asarray(tallies, jnp.int32))

    tallies = jnp.where(number % 4 == 0, named(packed, number // 4), named(ordinary, number - number // 4 - 1))
    mixed = jax.random.permutation(jax.random.fold_in(own, 3), count)
    donor, receiver = mixed[0:count // 2 * 2:2], mixed[1:count // 2 * 2:2]
    margin = jnp.minimum(tallies[donor] - 1, limit - tallies[receiver]) // 2
    margin = jnp.where((donor == order[0]) | (receiver == order[0]) | (tallies[receiver] == 0), 0, jnp.maximum(margin, 0))
    moved = jax.random.randint(jax.random.fold_in(own, 4), (count // 2,), 0, 1 << 20) % (margin + 1)
    tallies = tallies.at[donor].add(-moved).at[receiver].add(moved)
    labels = jnp.searchsorted(jnp.cumsum(tallies), jnp.arange(rows * top), side="right").astype(jnp.int32)
    table = labels.reshape(top, rows).T
    table = table[jax.random.permutation(jax.random.fold_in(own, 1), rows)]
    turn = jax.random.randint(jax.random.fold_in(own, 2), (rows, 1), 0, top)
    return jnp.take_along_axis(table, (jnp.arange(top)[None, :] + turn) % top, axis=1)


def portions_of(count, total, reach, lean, full):
    weights = [(1 << 20) // math.isqrt(grade ** lean) + 1 for grade in range(1, count + 1)]
    largest = reach if full else min(reach, max(-(-total // count), total * weights[0] // sum(weights)))
    least = 1 if total - largest >= count - 1 else 0
    holding, surplus = [largest] + [least] * (count - 1), total - largest - least * (count - 1)
    while surplus > 0:
        candidates = [i for i in range(1, count) if holding[i] < largest] or [i for i in range(1, count) if holding[i] < reach]
        mass, budget = sum([weights[i] for i in candidates]), surplus
        for i in candidates:
            extra = min(reach - holding[i], max(1, budget * weights[i] // mass), surplus)
            holding[i] = holding[i] + extra
            surplus = surplus - extra
    return np.array(holding)


def scatter_about(rng, shape, scale, bound, pieces=(), kind=jnp.bfloat16):
    loudness = levels(rng, shape, pieces, -0.22, 0.18) if pieces else 1.0
    drawn = jax.random.normal(rng, shape, jnp.float32) * scale * loudness
    return jnp.minimum(jnp.maximum(drawn, -bound), bound).astype(kind)


def bell_draw_with(own_key, dims, spread, bound, pieces, heavy, kind=jnp.bfloat16):
    values = spread * jax.random.normal(own_key, dims, jnp.float32)
    if pieces:
        values = values * levels(own_key, dims, pieces, -0.22, 0.18)
    return jnp.clip(spiked(values, jax.random.fold_in(own_key, 3), *heavy), -bound, bound).astype(kind)


def setup_inputs(seed: int = 0) -> dict:
    streams_of = jax.random.split(jax.random.key(seed), 16)
    resid = scatter_about(streams_of[0], (TOKEN_POSITIONS, D), 1.0, 6.0, ((0, 32),))
    norm_gain = jnp.clip(1.0 + 0.18 * jax.random.normal(streams_of[1], (D,), jnp.float32), 0.1, 1.9)
    cotangent = bell_draw_with(streams_of[2], (TOKEN_POSITIONS, D), 1.0, 6.0, ((0, 32),), (0, 1, 32, 2.75))
    route_ids_keys = jax.random.split(jax.random.fold_in(streams_of[3], 1), TOKEN_POSITIONS // TOK_DEV)
    route_ids_turns = jax.random.permutation(jax.random.fold_in(streams_of[3], 3), TOKEN_POSITIONS // TOK_DEV)
    route_ids = jax.vmap(lambda own, number: shared_out(jax.random.fold_in(streams_of[3], 2), own, number, TOK_DEV, EXPERTS, TOP, CAP, 2))(route_ids_keys, route_ids_turns).reshape((TOKEN_POSITIONS, TOP))
    route_weight = jnp.clip(0.25 + 2.0 * jax.random.uniform(streams_of[4], (TOKEN_POSITIONS, TOP), jnp.float32) ** levels(streams_of[4], (TOKEN_POSITIONS, TOP), ((0, 32),), -0.2, 0.2), 0.25, 2.25)
    expert_gate = scatter_about(streams_of[5], (EXPERTS, D, FE), D ** -0.5, 0.125, ((0, 32), (2, 16)))
    expert_up = scatter_about(streams_of[6], (EXPERTS, D, FE), D ** -0.5, 0.125, ((0, 32), (2, 16)))
    expert_down = scatter_about(streams_of[7], (EXPERTS, FE, D), FE ** -0.5, 0.125, ((0, 32), (1, 16)))
    out_proj = scatter_about(streams_of[8], (D, ATTENTION_HEADS * DV), (ATTENTION_HEADS * DV) ** -0.5, 0.09375, ((0, 32), (1, 16)))
    mixed = scatter_about(streams_of[9], (TOKEN_POSITIONS, ATTENTION_HEADS * DV), 1.0, 6.0, ((0, 32), (1, 16)))
    query = scatter_about(streams_of[10], (TOKEN_POSITIONS, ATTENTION_HEADS * KEY_CHANNELS), 1.0, 6.0, ((0, 32), (1, 16)))
    key = scatter_about(streams_of[11], (TOKEN_POSITIONS, ATTENTION_HEADS * KEY_CHANNELS), 0.25, 1.5, ((0, 32), (1, 16)))
    value = scatter_about(streams_of[12], (TOKEN_POSITIONS, ATTENTION_HEADS * DV), 1.0, 6.0, ((0, 32), (1, 16)))
    log_decay = draw_log_decay(jax.random.fold_in(streams_of[15], 71), 0)
    span_state = scatter_about(streams_of[14], (SPANS, ATTENTION_HEADS, KEY_CHANNELS, DV), 4.0, 24.0, ((0, 32), (1, 16)), jnp.float32)
    return {"resid": resid, "norm_gain": norm_gain, "cotangent": cotangent, "route_ids": route_ids, "route_weight": route_weight, "expert_gate": expert_gate, "expert_up": expert_up, "expert_down": expert_down, "out_proj": out_proj, "mixed": mixed, "query": query, "key": key, "value": value, "log_decay": log_decay, "span_state": span_state}


epsilon = 1e-06
highest = lax.Precision.HIGHEST

def rounded(values):
    return lax.optimization_barrier(values.astype(jnp.bfloat16)).astype(jnp.float32)

def into_blocks(values):
    return values.reshape(values.shape[0] // BLOCK, BLOCK, values.shape[1])

def span_forward(query_rows, key_rows, value_rows, grad_rows, decay_rows, entry_state):
    query_blk = into_blocks(query_rows)
    key_blk = into_blocks(key_rows)
    value_blk = into_blocks(value_rows)
    grad_blk = into_blocks(grad_rows)
    cumlog = jnp.cumsum(into_blocks(decay_rows), axis=1)
    block_total = cumlog[:, -1, :]
    to_end = jnp.exp(block_total[:, None, :] - cumlog)
    inner_part = jnp.einsum('nsd,nsj->ndj', key_blk * to_end, value_blk, precision=highest)

    def forward_step(carry_state, step_item):
        piece_part, block_sum = step_item
        return (jnp.exp(block_sum)[:, None] * carry_state + piece_part, carry_state)
    end_state, starts = lax.scan(forward_step, entry_state, (inner_part, block_total))
    own_part = jnp.einsum('ntd,ntj->ndj', query_blk * jnp.exp(cumlog), grad_blk, precision=highest)

    def backward_step(carry_state, step_item):
        piece_part, block_sum = step_item
        return (jnp.exp(block_sum)[:, None] * carry_state + piece_part, carry_state)
    start_cot, after_cot = lax.scan(backward_step, jnp.zeros_like(entry_state), (own_part, block_total), reverse=True)
    span_total = lax.optimization_barrier(jnp.sum(block_total, axis=0))
    later_log = span_total[None, :] - jnp.cumsum(block_total, axis=0)
    return ((cumlog, starts, after_cot, later_log, end_state), (jnp.exp(span_total), start_cot))

def span_backward(query_rows, key_rows, value_rows, grad_rows, kept_terms, exit_cot):
    cumlog, starts, after_cot, later_log, end_state = kept_terms
    query_blk = into_blocks(query_rows)
    key_blk = into_blocks(key_rows)
    value_blk = into_blocks(value_rows)
    grad_blk = into_blocks(grad_rows)
    exit_cots = after_cot + jnp.exp(later_log)[:, :, None] * exit_cot
    causal = jnp.arange(BLOCK)[:, None] >= jnp.arange(BLOCK)[None, :]
    decays = jnp.exp(jnp.where(causal[None, :, :, None], cumlog[:, :, None, :] - cumlog[:, None, :, :], -jnp.inf))
    scores = jnp.einsum('ntd,nsd,ntsd->nts', query_blk, key_blk, decays, precision=highest)
    grad_scores = jnp.einsum('ntj,nsj->nts', grad_blk, value_blk, precision=highest)
    grad_query = jnp.exp(cumlog) * jnp.einsum('ntj,ndj->ntd', grad_blk, starts, precision=highest)
    grad_query = grad_query + jnp.einsum('nts,nsd,ntsd->ntd', grad_scores, key_blk, decays, precision=highest)
    to_end = jnp.exp(cumlog[:, -1:, :] - cumlog)
    grad_key = jnp.einsum('nts,ntd,ntsd->nsd', grad_scores, query_blk, decays, precision=highest)
    grad_key = grad_key + to_end * jnp.einsum('nsj,ndj->nsd', value_blk, exit_cots, precision=highest)
    grad_value = jnp.einsum('nts,ntj->nsj', scores, grad_blk, precision=highest)
    grad_value = grad_value + jnp.einsum('nsd,ndj->nsj', key_blk * to_end, exit_cots, precision=highest)
    length = query_rows.shape[0]
    key_width = query_rows.shape[1]
    per_position = (query_blk * grad_query - key_blk * grad_key).reshape(length, key_width)
    grad_log = jnp.flip(jnp.cumsum(jnp.flip(per_position, 0), 0), 0) + lax.optimization_barrier(jnp.sum(end_state * exit_cot, axis=1))[None, :]
    return (grad_query.reshape(length, key_width), grad_key.reshape(length, key_width), grad_value.reshape(length, value_rows.shape[1]), grad_log)

def reference(resid, norm_gain, cotangent, route_ids, route_weight, expert_gate, expert_up, expert_down, out_proj, mixed, query, key, value, log_decay, span_state):
    resid_f = resid.astype(jnp.float32)
    inverse_rms = lax.rsqrt(lax.optimization_barrier(jnp.mean(resid_f * resid_f, axis=1, keepdims=True)) + epsilon)
    unit_rows = resid_f * inverse_rms
    normed = (unit_rows * norm_gain.astype(jnp.float32)).astype(jnp.bfloat16)
    sent_cot = (route_weight[:, :, None] * cotangent.astype(jnp.float32)[:, None, :]).astype(jnp.bfloat16)
    pair_expert = route_ids.reshape(N_SP, TOK_DEV * TOP)
    onehot = (pair_expert[:, :, None] == jnp.arange(EXPERTS, dtype=jnp.int32)[None, None, :]).astype(jnp.int32)
    slot_rank = lax.optimization_barrier(jnp.sum((jnp.cumsum(onehot, axis=1) - onehot) * onehot, axis=2))
    source = jnp.arange(N_SP, dtype=jnp.int32)[:, None]
    slot_index = ((pair_expert * N_SP + source) * CAP + slot_rank).astype(jnp.int32)
    pair_index = jnp.arange(TOKEN_POSITIONS * TOP, dtype=jnp.int32).reshape(N_SP, TOK_DEV * TOP)
    slot_table = jnp.full((EXPERTS * N_SP * CAP,), TOKEN_POSITIONS * TOP, jnp.int32)
    slot_table = slot_table.at[slot_index.reshape(-1)].set(pair_index.reshape(-1)).reshape(EXPERTS, N_SP * CAP)
    pair_rows = jnp.concatenate([jnp.repeat(normed, TOP, axis=0), jnp.zeros((1, D), jnp.bfloat16)], axis=0)
    pair_cots = jnp.concatenate([sent_cot.reshape(TOKEN_POSITIONS * TOP, D), jnp.zeros((1, D), jnp.bfloat16)], axis=0)
    group_width = FE // N_TP

    def one_expert(step_item):
        gate_w, up_w, down_w, slots = step_item
        rows_in = pair_rows[slots].astype(jnp.float32)
        rows_cot = pair_cots[slots].astype(jnp.float32)
        gate_f = gate_w.astype(jnp.float32)
        up_f = up_w.astype(jnp.float32)
        gate_pre = jnp.dot(rows_in, gate_f)
        up_pre = jnp.dot(rows_in, up_f)
        gate_sig = jax.nn.sigmoid(gate_pre)
        hidden = rounded(gate_pre * gate_sig * up_pre)
        grad_hidden = jnp.dot(rows_cot, down_w.astype(jnp.float32).T)
        grad_up_act = rounded(grad_hidden * gate_pre * gate_sig)
        grad_gate_act = rounded(grad_hidden * up_pre * gate_sig * (1.0 + gate_pre * (1.0 - gate_sig)))
        grad_down = jnp.dot(hidden.T, rows_cot).astype(jnp.bfloat16)
        grad_gate = jnp.dot(rows_in.T, grad_gate_act).astype(jnp.bfloat16)
        grad_up = jnp.dot(rows_in.T, grad_up_act).astype(jnp.bfloat16)
        rows_count = rows_in.shape[0]
        partial_value = jnp.einsum('rgf,dgf->grd', grad_gate_act.reshape(rows_count, N_TP, group_width), gate_f.reshape(D, N_TP, group_width))
        partial_value = partial_value + jnp.einsum('rgf,dgf->grd', grad_up_act.reshape(rows_count, N_TP, group_width), up_f.reshape(D, N_TP, group_width))
        pair_grad = lax.optimization_barrier(jnp.sum(rounded(partial_value), axis=0)).astype(jnp.bfloat16)
        return (grad_gate, grad_up, grad_down, pair_grad)
    grad_gate_all, grad_up_all, grad_down_all, pair_grads = lax.map(one_expert, (expert_gate, expert_up, expert_down, slot_table))
    pair_total = jnp.zeros((TOKEN_POSITIONS * TOP + 1, D), jnp.float32)
    pair_total = pair_total.at[slot_table.reshape(-1)].add(pair_grads.reshape(-1, D).astype(jnp.float32))
    grad_normed = lax.optimization_barrier(jnp.sum(pair_total[:-1].reshape(TOKEN_POSITIONS, TOP, D), axis=1))
    scaled = grad_normed * norm_gain.astype(jnp.float32)
    grad_resid = cotangent.astype(jnp.float32) + inverse_rms * (scaled - unit_rows * lax.optimization_barrier(jnp.mean(scaled * unit_rows, axis=1, keepdims=True)))
    grad_resid = grad_resid.astype(jnp.bfloat16)
    grad_out_proj = jnp.dot(grad_resid.T, mixed, preferred_element_type=jnp.float32)
    grad_mixed = jnp.dot(grad_resid, out_proj, preferred_element_type=jnp.float32).astype(jnp.bfloat16)
    query_scale = KEY_CHANNELS ** (-0.5)

    def heads_first(values, head_depth):
        return values.reshape(N_SP, TOK_DEV, ATTENTION_HEADS, head_depth).transpose(2, 0, 1, 3)

    def head_grads(step_item):
        query_h, key_h, value_h, grad_h, decay_h, state_h = step_item

        def span_step(exit_cot, span_item):
            query_p, key_p, value_p, grad_p, decay_p, entry_state = span_item
            query_rows = query_p.astype(jnp.float32) * query_scale
            key_rows = key_p.astype(jnp.float32)
            value_rows = value_p.astype(jnp.float32)
            grad_rows = grad_p.astype(jnp.float32)
            kept_terms, summary = span_forward(query_rows, key_rows, value_rows, grad_rows, decay_p, entry_state)
            span_grads = span_backward(query_rows, key_rows, value_rows, grad_rows, kept_terms, exit_cot)
            return (summary[0][:, None] * exit_cot + summary[1], span_grads)
        carry_end, span_grads = lax.scan(span_step, jnp.zeros((KEY_CHANNELS, DV), jnp.float32), (query_h, key_h, value_h, grad_h, decay_h, state_h), reverse=True)
        return span_grads
    grads_query, grads_key, grads_value, grads_log = lax.map(head_grads, (heads_first(query, KEY_CHANNELS), heads_first(key, KEY_CHANNELS), heads_first(value, DV), heads_first(grad_mixed, DV), heads_first(log_decay, KEY_CHANNELS), span_state.transpose(1, 0, 2, 3)))

    def tokens_first(values):
        return values.transpose(1, 2, 0, 3).reshape(TOKEN_POSITIONS, -1)
    grad_query = (tokens_first(grads_query) * query_scale).astype(jnp.bfloat16)
    grad_key = tokens_first(grads_key).astype(jnp.bfloat16)
    grad_value = tokens_first(grads_value).astype(jnp.bfloat16)
    grad_log_decay = tokens_first(grads_log)
    return (grad_gate_all, grad_up_all, grad_down_all, grad_out_proj, grad_query, grad_key, grad_value, grad_log_decay)
```

```python
import jax
import jax.numpy as jnp
from jax import lax
from jax.sharding import Mesh
from jax.sharding import PartitionSpec as P

KEY_CHANNELS = 128
DV = 256
TOP = 2
BLOCK = 64
SP = ("z", "x")
TP = ("y", "c")


epsilon = 1e-06


def sum_parts(tiles):
    return jnp.sum(tiles.astype(jnp.float32), axis=0)


def later_sum(states, decays, place):
    count = states.shape[0]
    total = jnp.zeros(states.shape[1:], jnp.float32)
    factor = jnp.ones(decays.shape[1:], jnp.float32)
    for k in range(count):
        later = k > place
        total = total + jnp.where(later, factor, 0.0)[:, None] * states[k].astype(jnp.float32)
        factor = jnp.where(later, factor * decays[k], factor)
    return total, factor


def to_all(array, axis):
    count = lax.axis_size(axis)
    copies = jnp.broadcast_to(array[None], (count, *array.shape))
    return lax.all_to_all(copies, axis, 0, 0, tiled=True)


def with_decay(state, decay):
    row = jnp.pad(decay[None, :], ((0, 7), (0, DV - KEY_CHANNELS)))
    return jnp.concatenate([state, row], axis=0).astype(jnp.bfloat16)


def split_decay(filled):
    decays = filled[:, KEY_CHANNELS, :KEY_CHANNELS].astype(jnp.float32)
    return filled[:, :KEY_CHANNELS], decays


def into_blocks(values):
    return values.reshape(values.shape[0] // BLOCK, BLOCK, values.shape[1])


def span_forward(query_rows, key_rows, value_rows, grad_rows, decay_rows, entry_state):
    query_blk = into_blocks(query_rows)
    key_blk = into_blocks(key_rows)
    value_blk = into_blocks(value_rows)
    grad_blk = into_blocks(grad_rows)
    cumlog = jnp.cumsum(into_blocks(decay_rows), axis=1)
    block_total = cumlog[:, -1, :]
    to_end = jnp.exp(block_total[:, None, :] - cumlog)
    inner_part = jnp.einsum("nsd,nsj->ndj", key_blk * to_end, value_blk)

    def forward_step(carry_state, step_item):
        piece_part, block_sum = step_item
        return (jnp.exp(block_sum)[:, None] * carry_state + piece_part, carry_state)

    end_state, starts = lax.scan(forward_step, entry_state, (inner_part, block_total))
    own_part = jnp.einsum("ntd,ntj->ndj", query_blk * jnp.exp(cumlog), grad_blk)

    def backward_step(carry_state, step_item):
        piece_part, block_sum = step_item
        return (jnp.exp(block_sum)[:, None] * carry_state + piece_part, carry_state)

    start_cot, after_cot = lax.scan(
        backward_step, jnp.zeros_like(entry_state), (own_part, block_total), reverse=True
    )
    span_total = jnp.sum(block_total, axis=0)
    later_log = span_total[None, :] - jnp.cumsum(block_total, axis=0)
    return ((cumlog, starts, after_cot, later_log, end_state), (jnp.exp(span_total), start_cot))


def span_backward(query_rows, key_rows, value_rows, grad_rows, kept_terms, exit_cot):
    cumlog, starts, after_cot, later_log, end_state = kept_terms
    query_blk = into_blocks(query_rows)
    key_blk = into_blocks(key_rows)
    value_blk = into_blocks(value_rows)
    grad_blk = into_blocks(grad_rows)
    exit_cots = after_cot + jnp.exp(later_log)[:, :, None] * exit_cot
    causal = jnp.arange(BLOCK)[:, None] >= jnp.arange(BLOCK)[None, :]
    decays = jnp.exp(
        jnp.where(causal[None, :, :, None], cumlog[:, :, None, :] - cumlog[:, None, :, :], -jnp.inf)
    )
    scores = jnp.einsum("ntd,nsd,ntsd->nts", query_blk, key_blk, decays)
    grad_scores = jnp.einsum("ntj,nsj->nts", grad_blk, value_blk)
    grad_query = jnp.exp(cumlog) * jnp.einsum("ntj,ndj->ntd", grad_blk, starts)
    grad_query = grad_query + jnp.einsum("nts,nsd,ntsd->ntd", grad_scores, key_blk, decays)
    to_end = jnp.exp(cumlog[:, -1:, :] - cumlog)
    grad_key = jnp.einsum("nts,ntd,ntsd->nsd", grad_scores, query_blk, decays)
    grad_key = grad_key + to_end * jnp.einsum("nsj,ndj->nsd", value_blk, exit_cots)
    grad_value = jnp.einsum("nts,ntj->nsj", scores, grad_blk)
    grad_value = grad_value + jnp.einsum("nsd,ndj->nsj", key_blk * to_end, exit_cots)
    length = query_rows.shape[0]
    key_width = query_rows.shape[1]
    per_position = (query_blk * grad_query - key_blk * grad_key).reshape(length, key_width)
    grad_log = (
        jnp.flip(jnp.cumsum(jnp.flip(per_position, 0), 0), 0)
        + jnp.sum(end_state * exit_cot, axis=1)[None, :]
    )
    return (
        grad_query.reshape(length, key_width),
        grad_key.reshape(length, key_width),
        grad_value.reshape(length, value_rows.shape[1]),
        grad_log,
    )


def on_device(
    resid,
    norm_gain,
    cotangent,
    route_ids,
    route_weight,
    expert_gate,
    expert_up,
    expert_down,
    out_proj,
    mixed,
    query,
    key,
    value,
    log_decay,
    span_state,
):
    tokens_here = resid.shape[0]
    model_width = resid.shape[1]
    half = model_width // 2
    sp_count = lax.axis_size(SP)
    y_count = lax.axis_size("y")
    experts = sp_count * expert_gate.shape[0]
    capacity = 3 * tokens_here // experts
    slots = experts * capacity
    core = lax.axis_index("c")
    resid_f = resid.astype(jnp.float32)
    inverse_rms = lax.rsqrt(jnp.mean(resid_f * resid_f, axis=1, keepdims=True) + epsilon)
    unit_rows = resid_f * inverse_rms
    normed = (unit_rows * norm_gain).astype(jnp.bfloat16)
    pair_expert = route_ids.reshape(-1)
    onehot = (pair_expert[:, None] == jnp.arange(experts, dtype=jnp.int32)[None, :]).astype(
        jnp.int32
    )
    slot_rank = jnp.sum((jnp.cumsum(onehot, axis=0) - onehot) * onehot, axis=1)
    slot_of = (pair_expert * capacity + slot_rank).reshape(tokens_here, TOP)
    slot_a, slot_b = slot_of[:, 0], slot_of[:, 1]
    packed = lax.broadcasted_iota(jnp.int32, (2 * slots, 2 * tokens_here), 0)
    aim_a = jnp.concatenate([2 * slot_a, 2 * slot_a + 1])[None, :]
    aim_b = jnp.concatenate([2 * slot_b, 2 * slot_b + 1])[None, :]
    hit_a, hit_b = packed == aim_a, packed == aim_b
    weight_a = jnp.concatenate([route_weight[:, 0]] * 2)[None, :]
    weight_b = jnp.concatenate([route_weight[:, 1]] * 2)[None, :]
    slot_weight = jnp.sum(
        jnp.where(hit_a, weight_a, 0.0) + jnp.where(hit_b, weight_b, 0.0), axis=1, keepdims=True
    )
    scale = jnp.where(core == 0, 1.0, slot_weight)
    chosen = jnp.where(core == 0, normed, cotangent)
    rows_two = jnp.concatenate([chosen[:, :half], chosen[:, half:]], axis=0)
    sent = jnp.dot((hit_a | hit_b).astype(jnp.bfloat16), rows_two, preferred_element_type=jnp.float32)
    sent = (sent * scale).astype(jnp.bfloat16).reshape(sp_count, 2 * capacity, half)
    own = lax.all_to_all(sent, SP, 0, 0, tiled=True).reshape(2 * slots, half)
    other = lax.ppermute(own, "c", [(0, 1), (1, 0)])
    rows_in = jnp.where(core == 0, own, other)
    rows_cot = jnp.where(core == 0, other, own)

    gate_w, up_w, down_w = expert_gate[0], expert_up[0], expert_down[0]
    width = gate_w.shape[1]
    into_w = jnp.concatenate([gate_w[:half], gate_w[half:], up_w[:half], up_w[half:]], axis=1)
    down_two = jnp.concatenate([down_w[:, :half], down_w[:, half:]], axis=0)
    pre = jnp.dot(rows_in, into_w, preferred_element_type=jnp.float32)
    gate_pre = pre[:, :width] + jnp.roll(pre[:, width : 2 * width], -1, axis=0)
    up_pre = pre[:, 2 * width : 3 * width] + jnp.roll(pre[:, 3 * width :], -1, axis=0)
    hid = lax.dot_general(
        rows_cot, down_two, (((1,), (1,)), ((), ())), preferred_element_type=jnp.float32
    )
    grad_hidden = hid[:, :width] + jnp.roll(hid[:, width:], -1, axis=0)
    gate_sig = jax.nn.sigmoid(gate_pre)
    first = (lax.broadcasted_iota(jnp.int32, (2 * slots, 1), 0) % 2) == 0

    def kept(values):
        return jnp.where(first, values, 0.0).astype(jnp.bfloat16)

    hidden = kept(gate_pre * gate_sig * up_pre)
    grad_up_act = kept(grad_hidden * gate_pre * gate_sig)
    grad_gate_act = kept(grad_hidden * up_pre * gate_sig * (1.0 + gate_pre * (1.0 - gate_sig)))
    acts = jnp.concatenate([grad_gate_act, grad_up_act], axis=1)
    pick = (
        lax.broadcasted_iota(jnp.int32, (slots, 2 * slots), 1)
        == 2 * lax.broadcasted_iota(jnp.int32, (slots, 2 * slots), 0)
    ).astype(jnp.bfloat16)
    acts = jnp.dot(pick, acts, preferred_element_type=jnp.float32).astype(jnp.bfloat16)
    out_w = jnp.concatenate([gate_w, up_w], axis=1).reshape(y_count, 2, width, 2 * width)
    out_own = jnp.where(core == 0, out_w[:, 0], out_w[:, 1]).reshape(half, 2 * width)
    out_other = jnp.where(core == 0, out_w[:, 1], out_w[:, 0]).reshape(half, 2 * width)

    def onto(weights):
        return lax.dot_general(
            acts, weights, (((1,), (1,)), ((), ())), preferred_element_type=jnp.float32
        )

    passed = lax.ppermute(onto(out_other).astype(jnp.bfloat16), "c", [(0, 1), (1, 0)])
    pair_sum = (onto(out_own) + passed.astype(jnp.float32)).astype(jnp.bfloat16)
    parts = pair_sum.reshape(slots, y_count, width).transpose(1, 0, 2)
    summed = sum_parts(lax.all_to_all(parts, "y", 0, 0, tiled=True)).astype(jnp.bfloat16)

    def beside(values):
        return jnp.concatenate([values, jnp.roll(values, 1, axis=0)], axis=1)

    grad_in_w = lax.dot_general(
        rows_in,
        jnp.concatenate([beside(grad_gate_act), beside(grad_up_act)], axis=1),
        (((0,), (0,)), ((), ())),
        preferred_element_type=jnp.float32,
    ).astype(jnp.bfloat16)
    grad_gate_w = jnp.concatenate([grad_in_w[:, :width], grad_in_w[:, width : 2 * width]], axis=0)
    grad_up_w = jnp.concatenate(
        [grad_in_w[:, 2 * width : 3 * width], grad_in_w[:, 3 * width :]], axis=0
    )
    grad_out_w = lax.dot_general(
        beside(hidden), rows_cot, (((0,), (0,)), ((), ())), preferred_element_type=jnp.float32
    ).astype(jnp.bfloat16)
    grad_down_w = jnp.concatenate([grad_out_w[:width], grad_out_w[width:]], axis=1)

    out_proj_here, own_tied = lax.optimization_barrier((out_proj, rows_in))
    out_proj_all = to_all(out_proj_here, SP).reshape(model_width, -1)

    returned = lax.all_to_all(
        summed.reshape(experts, capacity, -1), SP, split_axis=0, concat_axis=0, tiled=True
    )
    flat_rows = returned.reshape(slots, -1)
    slot_index = lax.broadcasted_iota(jnp.int32, (slots, tokens_here), 0)
    slot_tokens = ((slot_index == slot_a[None, :]) | (slot_index == slot_b[None, :])).astype(
        jnp.bfloat16
    )
    grad_normed = lax.all_gather(
        lax.dot_general(
            slot_tokens, flat_rows, (((0,), (0,)), ((), ())), preferred_element_type=jnp.float32
        ).astype(jnp.bfloat16),
        ("y", "c"),
        axis=1,
        tiled=True,
    ).astype(jnp.float32)
    scaled = grad_normed * norm_gain
    grad_resid = cotangent.astype(jnp.float32) + inverse_rms * (
        scaled - unit_rows * jnp.mean(scaled * unit_rows, axis=1, keepdims=True)
    )
    grad_resid = grad_resid.astype(jnp.bfloat16)
    grad_mixed = jnp.dot(grad_resid, out_proj_all, preferred_element_type=jnp.float32).astype(
        jnp.bfloat16
    )
    share = lax.dot_general(
        grad_resid, mixed, (((0,), (0,)), ((), ())), preferred_element_type=jnp.float32
    ).astype(jnp.bfloat16)
    grad_out_proj = sum_parts(
        lax.all_to_all(
            share.reshape(sp_count, model_width // sp_count, -1), SP, 0, 0, tiled=True
        )
    )
    head_count = query.shape[1] // KEY_CHANNELS
    query_scale = KEY_CHANNELS ** (-0.5)

    def heads_first(values, head_depth):
        return values.reshape(tokens_here, head_count, head_depth).transpose(1, 0, 2)

    query_rows = heads_first(query, KEY_CHANNELS).astype(jnp.float32) * query_scale
    key_rows = heads_first(key, KEY_CHANNELS).astype(jnp.float32)
    value_rows = heads_first(value, DV).astype(jnp.float32)
    grad_rows = heads_first(grad_mixed, DV).astype(jnp.float32)
    decay_rows = heads_first(log_decay, KEY_CHANNELS)
    kept_terms, summary = jax.vmap(span_forward)(
        query_rows, key_rows, value_rows, grad_rows, decay_rows, span_state[0]
    )
    own_decay, own_state = summary[0][0], summary[1][0]
    near_states, near_decays = split_decay(to_all(with_decay(own_state, own_decay), "x"))
    near_sum, near_factor = later_sum(near_states, near_decays, lax.axis_index("x"))
    group_sum, group_factor = later_sum(near_states, near_decays, -1)
    far_states, far_decays = split_decay(to_all(with_decay(group_sum, group_factor), "z"))
    far_sum, _ = later_sum(far_states, far_decays, lax.axis_index("z"))
    exit_cot = near_sum + near_factor[:, None] * far_sum
    head_grads = jax.vmap(span_backward)(
        query_rows, key_rows, value_rows, grad_rows, kept_terms, exit_cot[None]
    )

    def tokens_first(values):
        return values.transpose(1, 0, 2).reshape(tokens_here, -1)

    grad_query = (tokens_first(head_grads[0]) * query_scale).astype(jnp.bfloat16)
    grad_key = tokens_first(head_grads[1]).astype(jnp.bfloat16)
    grad_value = tokens_first(head_grads[2]).astype(jnp.bfloat16)
    grad_log_decay = tokens_first(head_grads[3])
    return (
        grad_gate_w[None],
        grad_up_w[None],
        grad_down_w[None],
        grad_out_proj,
        grad_query,
        grad_key,
        grad_value,
        grad_log_decay,
    )


def solution(mesh):
    finer = Mesh(mesh.devices.reshape(8, 4, 8, 2), ("z", "x", "y", "c"))
    in_specs = (
        P(SP, None),
        P(),
        P(SP, None),
        P(SP, None),
        P(SP, None),
        P(SP, None, TP),
        P(SP, None, TP),
        P(SP, TP, None),
        P(SP, TP),
        P(SP, TP),
        P(SP, TP),
        P(SP, TP),
        P(SP, TP),
        P(SP, TP),
        P(SP, TP, None, None),
    )
    out_specs = (
        P(SP, None, TP),
        P(SP, None, TP),
        P(SP, TP, None),
        P(SP, TP),
        P(SP, TP),
        P(SP, TP),
        P(SP, TP),
        P(SP, TP),
    )
    return jax.shard_map(
        on_device, mesh=finer, in_specs=in_specs, out_specs=out_specs, check_vma=False
    )
```

```python
import jax
import jax.numpy as jnp
from jax import lax
from jax.sharding import Mesh
from jax.sharding import PartitionSpec as P


KEY_CHANNELS = 128
DV = 256
TOP = 2
BLOCK = 64
SP = ("z", "x")
TP = ("y", "c")


epsilon = 1e-06


def sum_parts(tiles):
    return jnp.sum(tiles.astype(jnp.float32), axis=0)


def later_sum(states, decays, place):
    count = states.shape[0]
    total = jnp.zeros(states.shape[1:], jnp.float32)
    factor = jnp.ones(decays.shape[1:], jnp.float32)
    for k in range(count):
        later = k > place
        total = total + jnp.where(later, factor, 0.0)[:, None] * states[k].astype(jnp.float32)
        factor = jnp.where(later, factor * decays[k], factor)
    return total, factor


def named_dot(left, right):
    return lax.dot_general(
        left, right, (((0,), (0,)), ((), ())), preferred_element_type=jnp.float32
    ).astype(jnp.bfloat16)


def to_all(array, axis):
    count = lax.axis_size(axis)
    copies = jnp.broadcast_to(array[None], (count, *array.shape))
    return lax.all_to_all(copies, axis, 0, 0, tiled=True)


def with_decay(state, decay):
    row = jnp.pad(decay[None, :], ((0, 7), (0, DV - KEY_CHANNELS)))
    return jnp.concatenate([state, row], axis=0).astype(jnp.bfloat16)


def split_decay(filled):
    decays = filled[:, KEY_CHANNELS, :KEY_CHANNELS].astype(jnp.float32)
    return filled[:, :KEY_CHANNELS], decays


def into_blocks(values):
    return values.reshape(values.shape[0] // BLOCK, BLOCK, values.shape[1])


def span_forward(query_rows, key_rows, value_rows, grad_rows, decay_rows, entry_state):
    query_blk = into_blocks(query_rows)
    key_blk = into_blocks(key_rows)
    value_blk = into_blocks(value_rows)
    grad_blk = into_blocks(grad_rows)
    cumlog = jnp.cumsum(into_blocks(decay_rows), axis=1)
    block_total = cumlog[:, -1, :]
    to_end = jnp.exp(block_total[:, None, :] - cumlog)
    inner_part = jnp.einsum("nsd,nsj->ndj", key_blk * to_end, value_blk)

    def forward_step(carry_state, step_item):
        piece_part, block_sum = step_item
        return (jnp.exp(block_sum)[:, None] * carry_state + piece_part, carry_state)

    end_state, starts = lax.scan(
        forward_step, entry_state, (inner_part, block_total), unroll=True
    )
    own_part = jnp.einsum("ntd,ntj->ndj", query_blk * jnp.exp(cumlog), grad_blk)

    def backward_step(carry_state, step_item):
        piece_part, block_sum = step_item
        return (jnp.exp(block_sum)[:, None] * carry_state + piece_part, carry_state)

    start_cot, after_cot = lax.scan(
        backward_step,
        jnp.zeros_like(entry_state),
        (own_part, block_total),
        reverse=True,
        unroll=True,
    )
    span_total = jnp.sum(block_total, axis=0)
    later_log = span_total[None, :] - jnp.cumsum(block_total, axis=0)
    return ((cumlog, starts, after_cot, later_log, end_state), (jnp.exp(span_total), start_cot))


def span_backward(query_rows, key_rows, value_rows, grad_rows, kept_terms, exit_cot):
    cumlog, starts, after_cot, later_log, end_state = kept_terms
    query_blk = into_blocks(query_rows)
    key_blk = into_blocks(key_rows)
    value_blk = into_blocks(value_rows)
    grad_blk = into_blocks(grad_rows)
    exit_cots = after_cot + jnp.exp(later_log)[:, :, None] * exit_cot
    causal = jnp.arange(BLOCK)[:, None] >= jnp.arange(BLOCK)[None, :]
    decays = jnp.exp(
        jnp.where(causal[None, :, :, None], cumlog[:, :, None, :] - cumlog[:, None, :, :], -jnp.inf)
    )
    scores = jnp.einsum("ntd,nsd,ntsd->nts", query_blk, key_blk, decays)
    grad_scores = jnp.einsum("ntj,nsj->nts", grad_blk, value_blk)
    grad_query = jnp.exp(cumlog) * jnp.einsum("ntj,ndj->ntd", grad_blk, starts)
    grad_query = grad_query + jnp.einsum("nts,nsd,ntsd->ntd", grad_scores, key_blk, decays)
    to_end = jnp.exp(cumlog[:, -1:, :] - cumlog)
    grad_key = jnp.einsum("nts,ntd,ntsd->nsd", grad_scores, query_blk, decays)
    grad_key = grad_key + to_end * jnp.einsum("nsj,ndj->nsd", value_blk, exit_cots)
    grad_value = jnp.einsum("nts,ntj->nsj", scores, grad_blk)
    grad_value = grad_value + jnp.einsum("nsd,ndj->nsj", key_blk * to_end, exit_cots)
    length = query_rows.shape[0]
    key_width = query_rows.shape[1]
    per_position = (query_blk * grad_query - key_blk * grad_key).reshape(length, key_width)
    grad_log = (
        jnp.flip(jnp.cumsum(jnp.flip(per_position, 0), 0), 0)
        + jnp.sum(end_state * exit_cot, axis=1)[None, :]
    )
    return (
        grad_query.reshape(length, key_width),
        grad_key.reshape(length, key_width),
        grad_value.reshape(length, value_rows.shape[1]),
        grad_log,
    )


def on_device_body(
    resid,
    norm_gain,
    cotangent,
    route_ids,
    route_weight,
    expert_gate,
    expert_up,
    expert_down,
    out_proj,
    mixed,
    query,
    key,
    value,
    log_decay,
    span_state,
):
    tokens_here = resid.shape[0]
    model_width = resid.shape[1]
    half = model_width // 2
    sp_count = lax.axis_size(SP)
    y_count = lax.axis_size("y")
    experts = sp_count * expert_gate.shape[0]
    capacity = 3 * tokens_here // experts
    slots = experts * capacity
    core = lax.axis_index("c")
    resid_f = resid.astype(jnp.float32)
    inverse_rms = lax.rsqrt(jnp.mean(resid_f * resid_f, axis=1, keepdims=True) + epsilon)
    unit_rows = resid_f * inverse_rms
    normed = (unit_rows * norm_gain).astype(jnp.bfloat16)
    pair_expert = route_ids.reshape(-1)
    onehot = (pair_expert[:, None] == jnp.arange(experts, dtype=jnp.int32)[None, :]).astype(
        jnp.int32
    )
    slot_rank = jnp.sum((jnp.cumsum(onehot, axis=0) - onehot) * onehot, axis=1)
    slot_of = (pair_expert * capacity + slot_rank).reshape(tokens_here, TOP)
    slot_a, slot_b = slot_of[:, 0], slot_of[:, 1]
    packed = lax.broadcasted_iota(jnp.int32, (2 * slots, 2 * tokens_here), 0)
    aim_a = jnp.concatenate([2 * slot_a, 2 * slot_a + 1])[None, :]
    aim_b = jnp.concatenate([2 * slot_b, 2 * slot_b + 1])[None, :]
    hit_a, hit_b = packed == aim_a, packed == aim_b
    weight_a = jnp.concatenate([route_weight[:, 0]] * 2)[None, :]
    weight_b = jnp.concatenate([route_weight[:, 1]] * 2)[None, :]
    slot_weight = jnp.sum(
        jnp.where(hit_a, weight_a, 0.0) + jnp.where(hit_b, weight_b, 0.0), axis=1, keepdims=True
    )
    scale = jnp.where(core == 0, 1.0, slot_weight)
    chosen = jnp.where(core == 0, normed, cotangent)
    rows_two = jnp.concatenate([chosen[:, :half], chosen[:, half:]], axis=0)
    sent = jnp.dot((hit_a | hit_b).astype(jnp.bfloat16), rows_two, preferred_element_type=jnp.float32)
    sent = (sent * scale).astype(jnp.bfloat16).reshape(sp_count, 2 * capacity, half)
    own = lax.all_to_all(sent, SP, 0, 0, tiled=True).reshape(2 * slots, half)
    proj_near, _ = lax.optimization_barrier((out_proj, sent))
    proj_near = lax.all_gather(proj_near, "x", axis=0, tiled=True)
    other = lax.ppermute(own, "c", [(0, 1), (1, 0)])
    half_cols = out_proj.shape[1] // 2
    copies_a = jnp.broadcast_to(
        proj_near[None, :, :half_cols], (lax.axis_size("z"), proj_near.shape[0], half_cols)
    )
    copies_a, _ = lax.optimization_barrier((copies_a, own))
    proj_a = lax.all_to_all(copies_a, "z", 0, 0, tiled=True).reshape(model_width, half_cols)
    rows_in = jnp.where(core == 0, own, other)
    rows_cot = jnp.where(core == 0, other, own)

    gate_w, up_w, down_w = expert_gate[0], expert_up[0], expert_down[0]
    width = gate_w.shape[1]
    into_w = jnp.concatenate([gate_w[:half], gate_w[half:], up_w[:half], up_w[half:]], axis=1)
    down_two = jnp.concatenate([down_w[:, :half], down_w[:, half:]], axis=0)
    pre = jnp.dot(rows_in, into_w, preferred_element_type=jnp.float32)
    gate_pre = pre[:, :width] + jnp.roll(pre[:, width : 2 * width], -1, axis=0)
    up_pre = pre[:, 2 * width : 3 * width] + jnp.roll(pre[:, 3 * width :], -1, axis=0)
    hid = lax.dot_general(
        rows_cot, down_two, (((1,), (1,)), ((), ())), preferred_element_type=jnp.float32
    )
    grad_hidden = hid[:, :width] + jnp.roll(hid[:, width:], -1, axis=0)
    gate_sig = jax.nn.sigmoid(gate_pre)
    first = (lax.broadcasted_iota(jnp.int32, (2 * slots, 1), 0) % 2) == 0

    def kept(values):
        return jnp.where(first, values, 0.0).astype(jnp.bfloat16)

    hidden = kept(gate_pre * gate_sig * up_pre)
    grad_up_act = kept(grad_hidden * gate_pre * gate_sig)
    grad_gate_act = kept(grad_hidden * up_pre * gate_sig * (1.0 + gate_pre * (1.0 - gate_sig)))
    acts = jnp.concatenate([grad_gate_act, grad_up_act], axis=1)
    pick = (
        lax.broadcasted_iota(jnp.int32, (slots, 2 * slots), 1)
        == 2 * lax.broadcasted_iota(jnp.int32, (slots, 2 * slots), 0)
    ).astype(jnp.bfloat16)
    acts = jnp.dot(pick, acts, preferred_element_type=jnp.float32).astype(jnp.bfloat16)
    out_w = jnp.concatenate([gate_w, up_w], axis=1).reshape(y_count, 2, width, 2 * width)
    out_own = jnp.where(core == 0, out_w[:, 0], out_w[:, 1]).reshape(half, 2 * width)
    out_other = jnp.where(core == 0, out_w[:, 1], out_w[:, 0]).reshape(half, 2 * width)

    def onto(weights):
        return lax.dot_general(
            acts, weights, (((1,), (1,)), ((), ())), preferred_element_type=jnp.float32
        )

    passed = lax.ppermute(onto(out_other).astype(jnp.bfloat16), "c", [(0, 1), (1, 0)])
    pair_sum = (onto(out_own) + passed.astype(jnp.float32)).astype(jnp.bfloat16)
    parts = pair_sum.reshape(slots, y_count, width).transpose(1, 0, 2)
    swapped = lax.all_to_all(parts, "y", 0, 0, tiled=True)
    summed = sum_parts(swapped).astype(jnp.bfloat16)
    proj_b, _ = lax.optimization_barrier((proj_near[:, half_cols:], parts))
    proj_b = lax.all_gather(proj_b, "z", axis=0, tiled=True)
    out_proj_all = jnp.concatenate([proj_a, proj_b], axis=1)

    def beside(values):
        return jnp.concatenate([values, jnp.roll(values, 1, axis=0)], axis=1)

    grad_in_w = named_dot(
        rows_in,
        jnp.concatenate([beside(grad_gate_act), beside(grad_up_act)], axis=1),
    )
    grad_gate_w = jnp.concatenate([grad_in_w[:, :width], grad_in_w[:, width : 2 * width]], axis=0)
    grad_up_w = jnp.concatenate(
        [grad_in_w[:, 2 * width : 3 * width], grad_in_w[:, 3 * width :]], axis=0
    )
    grad_out_w = named_dot(beside(hidden), rows_cot)
    grad_down_w = jnp.concatenate([grad_out_w[:width], grad_out_w[width:]], axis=1)

    returned = lax.all_to_all(
        summed.reshape(experts, capacity, -1), SP, split_axis=0, concat_axis=0, tiled=True
    )
    flat_rows = returned.reshape(slots, -1)
    slot_index = lax.broadcasted_iota(jnp.int32, (slots, tokens_here), 0)
    slot_tokens = ((slot_index == slot_a[None, :]) | (slot_index == slot_b[None, :])).astype(
        jnp.bfloat16
    )
    grad_normed = lax.all_gather(
        lax.dot_general(
            slot_tokens, flat_rows, (((0,), (0,)), ((), ())), preferred_element_type=jnp.float32
        ).astype(jnp.bfloat16),
        ("y", "c"),
        axis=1,
        tiled=True,
    ).astype(jnp.float32)
    scaled = grad_normed * norm_gain
    grad_resid = cotangent.astype(jnp.float32) + inverse_rms * (
        scaled - unit_rows * jnp.mean(scaled * unit_rows, axis=1, keepdims=True)
    )
    grad_resid = grad_resid.astype(jnp.bfloat16)
    grad_mixed = jnp.dot(grad_resid, out_proj_all, preferred_element_type=jnp.float32).astype(
        jnp.bfloat16
    )
    share = lax.dot_general(
        grad_resid, mixed, (((0,), (0,)), ((), ())), preferred_element_type=jnp.float32
    ).astype(jnp.bfloat16)
    query_scale = KEY_CHANNELS ** (-0.5)
    query_rows = query.astype(jnp.float32) * query_scale
    key_rows = key.astype(jnp.float32)
    value_rows = value.astype(jnp.float32)
    grad_rows = grad_mixed.astype(jnp.float32)
    kept_terms, summary = span_forward(
        query_rows, key_rows, value_rows, grad_rows, log_decay, span_state[0, 0]
    )
    own_decay, own_state = summary
    near_states, near_decays = split_decay(to_all(with_decay(own_state, own_decay), "x"))
    near_sum, near_factor = later_sum(near_states, near_decays, lax.axis_index("x"))
    group_sum, group_factor = later_sum(near_states, near_decays, -1)
    far_filled = to_all(with_decay(group_sum, group_factor), "z")
    far_states, far_decays = split_decay(far_filled)
    z_count, x_count = lax.axis_size("z"), lax.axis_size("x")
    share_rows = model_width // sp_count
    share_x = share.reshape(z_count, x_count, share_rows, -1).transpose(1, 0, 2, 3)
    place = lax.axis_index("x")

    def for_place(k):
        return lax.dynamic_index_in_dim(share_x, jnp.bitwise_and(place + k, x_count - 1), 0, keepdims=False)

    share_sum = for_place(0).astype(jnp.float32)
    for k in range(1, 4):
        passed = lax.ppermute(
            for_place(k), "x", [(i, (i + k) % 4) for i in range(4)]
        )
        share_sum = share_sum + passed.astype(jnp.float32)
    share_z = share_sum.astype(jnp.bfloat16)
    share_z = lax.all_to_all(share_z, "z", 0, 0, tiled=True)
    grad_out_proj = sum_parts(share_z)
    far_sum, _ = later_sum(far_states, far_decays, lax.axis_index("z"))
    exit_cot = near_sum + near_factor[:, None] * far_sum
    grad_query, grad_key, grad_value, grad_log_decay = span_backward(
        query_rows, key_rows, value_rows, grad_rows, kept_terms, exit_cot
    )
    grad_query = (grad_query * query_scale).astype(jnp.bfloat16)
    grad_key = grad_key.astype(jnp.bfloat16)
    grad_value = grad_value.astype(jnp.bfloat16)
    return (
        grad_gate_w[None],
        grad_up_w[None],
        grad_down_w[None],
        grad_out_proj,
        grad_query,
        grad_key,
        grad_value,
        grad_log_decay,
    )


def solution(mesh):
    finer = Mesh(mesh.devices.reshape(8, 4, 8, 2), ("z", "x", "y", "c"))
    in_specs = (
        P(SP, None),
        P(),
        P(SP, None),
        P(SP, None),
        P(SP, None),
        P(SP, None, TP),
        P(SP, None, TP),
        P(SP, TP, None),
        P(SP, TP),
        P(SP, TP),
        P(SP, TP),
        P(SP, TP),
        P(SP, TP),
        P(SP, TP),
        P(SP, TP, None, None),
    )
    out_specs = (
        P(SP, None, TP),
        P(SP, None, TP),
        P(SP, TP, None),
        P(SP, TP),
        P(SP, TP),
        P(SP, TP),
        P(SP, TP),
        P(SP, TP),
    )
    return jax.shard_map(
        on_device_body, mesh=finer, in_specs=in_specs, out_specs=out_specs, check_vma=False
    )
```

```python
import jax
import jax.numpy as jnp
from jax import lax
from jax.sharding import Mesh
from jax.sharding import PartitionSpec as P


KEY_CHANNELS = 128
DV = 256
TOP = 2
BLOCK = 64
SP = ("z", "x")
TP = ("y", "c")


epsilon = 1e-06


def sum_parts(tiles):
    return jnp.sum(tiles.astype(jnp.float32), axis=0)


def later_sum(states, decays, place):
    count = states.shape[0]
    total = jnp.zeros(states.shape[1:], jnp.float32)
    factor = jnp.ones(decays.shape[1:], jnp.float32)
    for k in range(count):
        later = k > place
        total = total + jnp.where(later, factor, 0.0)[:, None] * states[k].astype(jnp.float32)
        factor = jnp.where(later, factor * decays[k], factor)
    return total, factor


def named_dot(left, right):
    return lax.dot_general(
        left, right, (((0,), (0,)), ((), ())), preferred_element_type=jnp.float32
    ).astype(jnp.bfloat16)


def to_all(array, axis):
    count = lax.axis_size(axis)
    copies = jnp.broadcast_to(array[None], (count, *array.shape))
    return lax.all_to_all(copies, axis, 0, 0, tiled=True)


def with_decay(state, decay):
    row = jnp.pad(decay[None, :], ((0, 7), (0, DV - KEY_CHANNELS)))
    return jnp.concatenate([state, row], axis=0).astype(jnp.bfloat16)


def split_decay(filled):
    decays = filled[:, KEY_CHANNELS, :KEY_CHANNELS].astype(jnp.float32)
    return filled[:, :KEY_CHANNELS], decays


def into_blocks(values):
    return values.reshape(values.shape[0] // BLOCK, BLOCK, values.shape[1])


def span_forward(query_rows, key_rows, value_rows, grad_rows, decay_rows, entry_state):
    query_blk = into_blocks(query_rows)
    key_blk = into_blocks(key_rows)
    value_blk = into_blocks(value_rows)
    grad_blk = into_blocks(grad_rows)
    cumlog = jnp.cumsum(into_blocks(decay_rows), axis=1)
    block_total = cumlog[:, -1, :]
    to_end = jnp.exp(block_total[:, None, :] - cumlog)
    inner_part = jnp.einsum("nsd,nsj->ndj", key_blk * to_end, value_blk)

    def forward_step(carry_state, step_item):
        piece_part, block_sum = step_item
        return (jnp.exp(block_sum)[:, None] * carry_state + piece_part, carry_state)

    end_state, starts = lax.scan(
        forward_step, entry_state, (inner_part, block_total), unroll=True
    )
    own_part = jnp.einsum("ntd,ntj->ndj", query_blk * jnp.exp(cumlog), grad_blk)

    def backward_step(carry_state, step_item):
        piece_part, block_sum = step_item
        return (jnp.exp(block_sum)[:, None] * carry_state + piece_part, carry_state)

    start_cot, after_cot = lax.scan(
        backward_step,
        jnp.zeros_like(entry_state),
        (own_part, block_total),
        reverse=True,
        unroll=True,
    )
    span_total = jnp.sum(block_total, axis=0)
    later_log = span_total[None, :] - jnp.cumsum(block_total, axis=0)
    return ((cumlog, starts, after_cot, later_log, end_state), (jnp.exp(span_total), start_cot))


def span_backward(query_rows, key_rows, value_rows, grad_rows, kept_terms, exit_cot):
    cumlog, starts, after_cot, later_log, end_state = kept_terms
    query_blk = into_blocks(query_rows)
    key_blk = into_blocks(key_rows)
    value_blk = into_blocks(value_rows)
    grad_blk = into_blocks(grad_rows)
    exit_cots = after_cot + jnp.exp(later_log)[:, :, None] * exit_cot
    causal = jnp.arange(BLOCK)[:, None] >= jnp.arange(BLOCK)[None, :]
    decays = jnp.exp(
        jnp.where(causal[None, :, :, None], cumlog[:, :, None, :] - cumlog[:, None, :, :], -jnp.inf)
    )
    scores = jnp.einsum("ntd,nsd,ntsd->nts", query_blk, key_blk, decays)
    grad_scores = jnp.einsum("ntj,nsj->nts", grad_blk, value_blk)
    grad_query = jnp.exp(cumlog) * jnp.einsum("ntj,ndj->ntd", grad_blk, starts)
    grad_query = grad_query + jnp.einsum("nts,nsd,ntsd->ntd", grad_scores, key_blk, decays)
    to_end = jnp.exp(cumlog[:, -1:, :] - cumlog)
    grad_key = jnp.einsum("nts,ntd,ntsd->nsd", grad_scores, query_blk, decays)
    grad_key = grad_key + to_end * jnp.einsum("nsj,ndj->nsd", value_blk, exit_cots)
    grad_value = jnp.einsum("nts,ntj->nsj", scores, grad_blk)
    grad_value = grad_value + jnp.einsum("nsd,ndj->nsj", key_blk * to_end, exit_cots)
    length = query_rows.shape[0]
    key_width = query_rows.shape[1]
    per_position = (query_blk * grad_query - key_blk * grad_key).reshape(length, key_width)
    grad_log = (
        jnp.flip(jnp.cumsum(jnp.flip(per_position, 0), 0), 0)
        + jnp.sum(end_state * exit_cot, axis=1)[None, :]
    )
    return (
        grad_query.reshape(length, key_width),
        grad_key.reshape(length, key_width),
        grad_value.reshape(length, value_rows.shape[1]),
        grad_log,
    )


def on_device_body(
    resid,
    norm_gain,
    cotangent,
    route_ids,
    route_weight,
    expert_gate,
    expert_up,
    expert_down,
    out_proj,
    mixed,
    query,
    key,
    value,
    log_decay,
    span_state,
):
    tokens_here = resid.shape[0]
    model_width = resid.shape[1]
    half = model_width // 2
    sp_count = lax.axis_size(SP)
    y_count = lax.axis_size("y")
    experts = sp_count * expert_gate.shape[0]
    capacity = 3 * tokens_here // experts
    slots = experts * capacity
    core = lax.axis_index("c")
    resid_f = resid.astype(jnp.float32)
    inverse_rms = lax.rsqrt(jnp.mean(resid_f * resid_f, axis=1, keepdims=True) + epsilon)
    unit_rows = resid_f * inverse_rms
    normed = (unit_rows * norm_gain).astype(jnp.bfloat16)
    pair_expert = route_ids.reshape(-1)
    onehot = (pair_expert[:, None] == jnp.arange(experts, dtype=jnp.int32)[None, :]).astype(
        jnp.int32
    )
    slot_rank = jnp.sum((jnp.cumsum(onehot, axis=0) - onehot) * onehot, axis=1)
    slot_of = (pair_expert * capacity + slot_rank).reshape(tokens_here, TOP)
    slot_a, slot_b = slot_of[:, 0], slot_of[:, 1]
    packed = lax.broadcasted_iota(jnp.int32, (2 * slots, 2 * tokens_here), 0)
    aim_a = jnp.concatenate([2 * slot_a, 2 * slot_a + 1])[None, :]
    aim_b = jnp.concatenate([2 * slot_b, 2 * slot_b + 1])[None, :]
    hit_a, hit_b = packed == aim_a, packed == aim_b
    weight_a = jnp.concatenate([route_weight[:, 0]] * 2)[None, :]
    weight_b = jnp.concatenate([route_weight[:, 1]] * 2)[None, :]
    slot_weight = jnp.sum(
        jnp.where(hit_a, weight_a, 0.0) + jnp.where(hit_b, weight_b, 0.0), axis=1, keepdims=True
    )
    scale = jnp.where(core == 0, 1.0, slot_weight)
    chosen = jnp.where(core == 0, normed, cotangent)
    rows_two = jnp.concatenate([chosen[:, :half], chosen[:, half:]], axis=0)
    sent = jnp.dot((hit_a | hit_b).astype(jnp.bfloat16), rows_two, preferred_element_type=jnp.float32)
    sent = (sent * scale).astype(jnp.bfloat16).reshape(sp_count, 2 * capacity, half)
    own = lax.all_to_all(sent, SP, 0, 0, tiled=True).reshape(2 * slots, half)
    proj_near, _ = lax.optimization_barrier((out_proj, sent))
    proj_near = lax.all_gather(proj_near, "x", axis=0, tiled=True)
    other = lax.ppermute(own, "c", [(0, 1), (1, 0)])
    rows_in = jnp.where(core == 0, own, other)
    rows_cot = jnp.where(core == 0, other, own)

    gate_w, up_w, down_w = expert_gate[0], expert_up[0], expert_down[0]
    width = gate_w.shape[1]
    into_w = jnp.concatenate([gate_w[:half], gate_w[half:], up_w[:half], up_w[half:]], axis=1)
    down_two = jnp.concatenate([down_w[:, :half], down_w[:, half:]], axis=0)
    pre = jnp.dot(rows_in, into_w, preferred_element_type=jnp.float32)
    gate_pre = pre[:, :width] + jnp.roll(pre[:, width : 2 * width], -1, axis=0)
    up_pre = pre[:, 2 * width : 3 * width] + jnp.roll(pre[:, 3 * width :], -1, axis=0)
    hid = lax.dot_general(
        rows_cot, down_two, (((1,), (1,)), ((), ())), preferred_element_type=jnp.float32
    )
    grad_hidden = hid[:, :width] + jnp.roll(hid[:, width:], -1, axis=0)
    gate_sig = jax.nn.sigmoid(gate_pre)
    first = (lax.broadcasted_iota(jnp.int32, (2 * slots, 1), 0) % 2) == 0

    def kept(values):
        return jnp.where(first, values, 0.0).astype(jnp.bfloat16)

    hidden = kept(gate_pre * gate_sig * up_pre)
    grad_up_act = kept(grad_hidden * gate_pre * gate_sig)
    grad_gate_act = kept(grad_hidden * up_pre * gate_sig * (1.0 + gate_pre * (1.0 - gate_sig)))
    acts = jnp.concatenate([grad_gate_act, grad_up_act], axis=1)
    pick = (
        lax.broadcasted_iota(jnp.int32, (slots, 2 * slots), 1)
        == 2 * lax.broadcasted_iota(jnp.int32, (slots, 2 * slots), 0)
    ).astype(jnp.bfloat16)
    acts = jnp.dot(pick, acts, preferred_element_type=jnp.float32).astype(jnp.bfloat16)
    out_w = jnp.concatenate([gate_w, up_w], axis=1).reshape(y_count, 2, width, 2 * width)
    out_own = jnp.where(core == 0, out_w[:, 0], out_w[:, 1]).reshape(half, 2 * width)
    out_other = jnp.where(core == 0, out_w[:, 1], out_w[:, 0]).reshape(half, 2 * width)

    def onto(weights):
        return lax.dot_general(
            acts, weights, (((1,), (1,)), ((), ())), preferred_element_type=jnp.float32
        )

    passed = lax.ppermute(onto(out_other).astype(jnp.bfloat16), "c", [(0, 1), (1, 0)])
    pair_sum = (onto(out_own) + passed.astype(jnp.float32)).astype(jnp.bfloat16)
    parts = pair_sum.reshape(slots, y_count, width).transpose(1, 0, 2)
    swapped = lax.all_to_all(parts, "y", 0, 0, tiled=True)
    summed = sum_parts(swapped).astype(jnp.bfloat16)
    proj_tied, _ = lax.optimization_barrier((proj_near, parts))
    z_place = lax.axis_index("z")
    blocks = [(0, proj_near)]
    for k in (1, 7, 2, 6, 3, 5, 4):
        ring = [(i, (i + k) % 8) for i in range(8)]
        blocks.append((k, lax.ppermute(proj_tied, "z", ring)))
    out_proj_all = jnp.zeros((model_width, out_proj.shape[1]), out_proj.dtype)
    for k, block in blocks:
        at = jnp.bitwise_and(z_place + (8 - k), 7) * block.shape[0]
        out_proj_all = lax.dynamic_update_slice(
            out_proj_all, block, (at.astype(jnp.uint32), jnp.uint32(0))
        )

    def beside(values):
        return jnp.concatenate([values, jnp.roll(values, 1, axis=0)], axis=1)

    grad_in_w = named_dot(
        rows_in,
        jnp.concatenate([beside(grad_gate_act), beside(grad_up_act)], axis=1),
    )
    grad_gate_w = jnp.concatenate([grad_in_w[:, :width], grad_in_w[:, width : 2 * width]], axis=0)
    grad_up_w = jnp.concatenate(
        [grad_in_w[:, 2 * width : 3 * width], grad_in_w[:, 3 * width :]], axis=0
    )
    grad_out_w = named_dot(beside(hidden), rows_cot)
    grad_down_w = jnp.concatenate([grad_out_w[:width], grad_out_w[width:]], axis=1)

    returned = lax.all_to_all(
        summed.reshape(experts, capacity, -1), SP, split_axis=0, concat_axis=0, tiled=True
    )
    flat_rows = returned.reshape(slots, -1)
    slot_index = lax.broadcasted_iota(jnp.int32, (slots, tokens_here), 0)
    slot_tokens = ((slot_index == slot_a[None, :]) | (slot_index == slot_b[None, :])).astype(
        jnp.bfloat16
    )
    grad_normed = lax.all_gather(
        lax.dot_general(
            slot_tokens, flat_rows, (((0,), (0,)), ((), ())), preferred_element_type=jnp.float32
        ).astype(jnp.bfloat16),
        ("y", "c"),
        axis=1,
        tiled=True,
    ).astype(jnp.float32)
    scaled = grad_normed * norm_gain
    grad_resid = cotangent.astype(jnp.float32) + inverse_rms * (
        scaled - unit_rows * jnp.mean(scaled * unit_rows, axis=1, keepdims=True)
    )
    grad_resid = grad_resid.astype(jnp.bfloat16)
    grad_mixed = jnp.dot(grad_resid, out_proj_all, preferred_element_type=jnp.float32).astype(
        jnp.bfloat16
    )
    share = lax.dot_general(
        grad_resid, mixed, (((0,), (0,)), ((), ())), preferred_element_type=jnp.float32
    ).astype(jnp.bfloat16)
    query_scale = KEY_CHANNELS ** (-0.5)
    query_rows = query.astype(jnp.float32) * query_scale
    key_rows = key.astype(jnp.float32)
    value_rows = value.astype(jnp.float32)
    grad_rows = grad_mixed.astype(jnp.float32)
    kept_terms, summary = span_forward(
        query_rows, key_rows, value_rows, grad_rows, log_decay, span_state[0, 0]
    )
    own_decay, own_state = summary
    near_states, near_decays = split_decay(to_all(with_decay(own_state, own_decay), "x"))
    near_sum, near_factor = later_sum(near_states, near_decays, lax.axis_index("x"))
    group_sum, group_factor = later_sum(near_states, near_decays, -1)
    far_filled = to_all(with_decay(group_sum, group_factor), "z")
    far_states, far_decays = split_decay(far_filled)
    z_count, x_count = lax.axis_size("z"), lax.axis_size("x")
    share_rows = model_width // sp_count
    share_x = share.reshape(z_count, x_count, share_rows, -1).transpose(1, 0, 2, 3)
    place = lax.axis_index("x")

    def for_place(k):
        at = jnp.bitwise_and(place + k, x_count - 1).astype(jnp.uint32)
        return lax.dynamic_index_in_dim(share_x, at, 0, keepdims=False)

    share_sum = for_place(0).astype(jnp.float32)
    for k in range(1, 4):
        passed = lax.ppermute(
            for_place(k), "x", [(i, (i + k) % 4) for i in range(4)]
        )
        share_sum = share_sum + passed.astype(jnp.float32)
    share_z = share_sum.astype(jnp.bfloat16)
    share_z = lax.all_to_all(share_z, "z", 0, 0, tiled=True)
    grad_out_proj = sum_parts(share_z)
    far_sum, _ = later_sum(far_states, far_decays, lax.axis_index("z"))
    exit_cot = near_sum + near_factor[:, None] * far_sum
    grad_query, grad_key, grad_value, grad_log_decay = span_backward(
        query_rows, key_rows, value_rows, grad_rows, kept_terms, exit_cot
    )
    grad_query = (grad_query * query_scale).astype(jnp.bfloat16)
    grad_key = grad_key.astype(jnp.bfloat16)
    grad_value = grad_value.astype(jnp.bfloat16)
    return (
        grad_gate_w[None],
        grad_up_w[None],
        grad_down_w[None],
        grad_out_proj,
        grad_query,
        grad_key,
        grad_value,
        grad_log_decay,
    )


def solution(mesh):
    finer = Mesh(mesh.devices.reshape(8, 4, 8, 2), ("z", "x", "y", "c"))
    in_specs = (
        P(SP, None),
        P(),
        P(SP, None),
        P(SP, None),
        P(SP, None),
        P(SP, None, TP),
        P(SP, None, TP),
        P(SP, TP, None),
        P(SP, TP),
        P(SP, TP),
        P(SP, TP),
        P(SP, TP),
        P(SP, TP),
        P(SP, TP),
        P(SP, TP, None, None),
    )
    out_specs = (
        P(SP, None, TP),
        P(SP, None, TP),
        P(SP, TP, None),
        P(SP, TP),
        P(SP, TP),
        P(SP, TP),
        P(SP, TP),
        P(SP, TP),
    )
    return jax.shard_map(
        on_device_body, mesh=finer, in_specs=in_specs, out_specs=out_specs, check_vma=False
    )
```

```python
import jax
import jax.numpy as jnp
from jax import lax
from jax.experimental import pallas as pl
from jax.experimental.pallas import tpu as pltpu
from jax.sharding import Mesh
from jax.sharding import PartitionSpec as P


KEY_CHANNELS = 128
DV = 256
CAPACITY = 12
BLOCK = 64
SP = ("z", "x")
TP = ("y", "c")


epsilon = 1e-06


def sum_parts(tiles):
    return jnp.sum(tiles.astype(jnp.float32), axis=0)


def later_sum(states, decays, place):
    count = states.shape[0]
    total = jnp.zeros(states.shape[1:], jnp.float32)
    factor = jnp.ones(decays.shape[1:], jnp.float32)
    for k in range(count):
        later = k > place
        total = total + jnp.where(later, factor, 0.0)[:, None] * states[k].astype(jnp.float32)
        factor = jnp.where(later, factor * decays[k], factor)
    return total, factor


def named_dot(left, right):
    return lax.dot_general(
        left, right, (((0,), (0,)), ((), ())), preferred_element_type=jnp.float32
    ).astype(jnp.bfloat16)


def to_all(array, axis):
    count = lax.axis_size(axis)
    copies = jnp.broadcast_to(array[None], (count, *array.shape))
    return lax.all_to_all(copies, axis, 0, 0, tiled=True)


def with_decay(state, decay):
    row = jnp.pad(decay[None, :], ((0, 7), (0, DV - KEY_CHANNELS)))
    return jnp.concatenate([state, row], axis=0).astype(jnp.bfloat16)


def split_decay(filled):
    decays = filled[:, KEY_CHANNELS, :KEY_CHANNELS].astype(jnp.float32)
    return filled[:, :KEY_CHANNELS], decays


def into_blocks(values):
    return values.reshape(values.shape[0] // BLOCK, BLOCK, values.shape[1])


def span_forward(query_rows, key_rows, value_rows, grad_rows, decay_rows, entry_state):
    query_blk = into_blocks(query_rows)
    key_blk = into_blocks(key_rows)
    value_blk = into_blocks(value_rows)
    grad_blk = into_blocks(grad_rows)
    cumlog = jnp.cumsum(into_blocks(decay_rows), axis=1)
    block_total = cumlog[:, -1, :]
    to_end = jnp.exp(block_total[:, None, :] - cumlog)
    inner_part = jnp.einsum("nsd,nsj->ndj", key_blk * to_end, value_blk)

    def forward_step(carry_state, step_item):
        piece_part, block_sum = step_item
        return (jnp.exp(block_sum)[:, None] * carry_state + piece_part, carry_state)

    end_state, starts = lax.scan(
        forward_step, entry_state, (inner_part, block_total), unroll=True
    )
    own_part = jnp.einsum("ntd,ntj->ndj", query_blk * jnp.exp(cumlog), grad_blk)

    def backward_step(carry_state, step_item):
        piece_part, block_sum = step_item
        return (jnp.exp(block_sum)[:, None] * carry_state + piece_part, carry_state)

    start_cot, after_cot = lax.scan(
        backward_step,
        jnp.zeros_like(entry_state),
        (own_part, block_total),
        reverse=True,
        unroll=True,
    )
    span_total = jnp.sum(block_total, axis=0)
    later_log = span_total[None, :] - jnp.cumsum(block_total, axis=0)
    return ((cumlog, starts, after_cot, later_log, end_state), (jnp.exp(span_total), start_cot))


def span_backward(query_rows, key_rows, value_rows, grad_rows, kept_terms, exit_cot):
    cumlog, starts, after_cot, later_log, end_state = kept_terms
    query_blk = into_blocks(query_rows)
    key_blk = into_blocks(key_rows)
    value_blk = into_blocks(value_rows)
    grad_blk = into_blocks(grad_rows)
    exit_cots = after_cot + jnp.exp(later_log)[:, :, None] * exit_cot
    causal = jnp.arange(BLOCK)[:, None] >= jnp.arange(BLOCK)[None, :]
    decays = jnp.exp(
        jnp.where(causal[None, :, :, None], cumlog[:, :, None, :] - cumlog[:, None, :, :], -jnp.inf)
    )
    scores = jnp.einsum("ntd,nsd,ntsd->nts", query_blk, key_blk, decays)
    grad_scores = jnp.einsum("ntj,nsj->nts", grad_blk, value_blk)
    grad_query = jnp.exp(cumlog) * jnp.einsum("ntj,ndj->ntd", grad_blk, starts)
    grad_query = grad_query + jnp.einsum("nts,nsd,ntsd->ntd", grad_scores, key_blk, decays)
    to_end = jnp.exp(cumlog[:, -1:, :] - cumlog)
    grad_key = jnp.einsum("nts,ntd,ntsd->nsd", grad_scores, query_blk, decays)
    grad_key = grad_key + to_end * jnp.einsum("nsj,ndj->nsd", value_blk, exit_cots)
    grad_value = jnp.einsum("nts,ntj->nsj", scores, grad_blk)
    grad_value = grad_value + jnp.einsum("nsd,ndj->nsj", key_blk * to_end, exit_cots)
    length = query_rows.shape[0]
    key_width = query_rows.shape[1]
    per_position = (query_blk * grad_query - key_blk * grad_key).reshape(length, key_width)
    grad_log = (
        jnp.flip(jnp.cumsum(jnp.flip(per_position, 0), 0), 0)
        + jnp.sum(end_state * exit_cot, axis=1)[None, :]
    )
    return (
        grad_query.reshape(length, key_width),
        grad_key.reshape(length, key_width),
        grad_value.reshape(length, value_rows.shape[1]),
        grad_log,
    )


def dispatch_rows_kernel(core_ref, ids_ref, weight_ref, resid_ref, cot_ref, gain_ref, sent_ref, slot_ref, rows_ref):
    tokens, model_width = resid_ref.shape
    half = model_width // 2
    experts = sent_ref.shape[0] // (2 * CAPACITY)

    square = (tokens, tokens)
    row_at = lax.broadcasted_iota(jnp.int32, square, 0)
    col_at = lax.broadcasted_iota(jnp.int32, square, 1)
    along = [ids_ref[k : k + 1, :].astype(jnp.float32) for k in range(2)]

    @pl.when(core_ref[0] == 0)
    def _():
        for at in range(0, tokens, 32):
            r = resid_ref[at : at + 32, :].astype(jnp.float32)
            inverse_rms = lax.rsqrt(jnp.mean(r * r, axis=1, keepdims=True) + epsilon)
            normed = (r * inverse_rms * gain_ref[...]).astype(jnp.bfloat16)
            for k in range(2):
                for h in range(2):
                    low = (2 * k + h) * tokens + at
                    rows_ref[low : low + 32, :] = normed[:, h * half : (h + 1) * half]

    @pl.when(core_ref[0] != 0)
    def _():
        weights = []
        for k in range(2):
            spread = jnp.broadcast_to(weight_ref[k : k + 1, :], square)
            weights.append(
                jnp.sum(jnp.where(row_at == col_at, spread, 0.0), axis=1, keepdims=True)
            )
        for at in range(0, tokens, 32):
            c = cot_ref[at : at + 32, :].astype(jnp.float32)
            for k in range(2):
                sent = (c * weights[k][at : at + 32, :]).astype(jnp.bfloat16)
                for h in range(2):
                    low = (2 * k + h) * tokens + at
                    rows_ref[low : low + 32, :] = sent[:, h * half : (h + 1) * half]

    expert_at = lax.broadcasted_iota(jnp.int32, (experts, tokens), 0).astype(jnp.float32)
    named = [(expert_at == a).astype(jnp.float32) for a in along]
    earlier = (row_at < col_at).astype(jnp.bfloat16)
    before = jnp.dot(
        (named[0] + named[1]).astype(jnp.bfloat16), earlier, preferred_element_type=jnp.float32
    )
    slots = [
        (a * CAPACITY + jnp.sum(n * before, axis=0, keepdims=True)).astype(jnp.int32)
        for a, n in zip(along, named)
    ]
    slot_ref[...] = jnp.concatenate(slots + [jnp.zeros((6, tokens), jnp.int32)], axis=0)
    step = 256
    for at in range(0, sent_ref.shape[0], step):
        packed = lax.broadcasted_iota(jnp.int32, (step, tokens), 0) + at
        hits = [
            jnp.where(packed == 2 * slot + h, 1.0, 0.0).astype(jnp.bfloat16)
            for slot in slots
            for h in range(2)
        ]
        sent_ref[at : at + step, :] = jnp.dot(
            jnp.concatenate(hits, axis=1), rows_ref[...], preferred_element_type=jnp.float32
        ).astype(jnp.bfloat16)


def dispatch_rows(core, ids, weight, resid, cotangent, gain, experts):
    tokens, model_width = resid.shape
    half = model_width // 2
    vmem = pl.BlockSpec(memory_space=pltpu.VMEM)
    return pl.pallas_call(
        dispatch_rows_kernel,
        out_shape=(
            jax.ShapeDtypeStruct((2 * experts * CAPACITY, half), jnp.bfloat16),
            jax.ShapeDtypeStruct((8, tokens), jnp.int32),
        ),
        in_specs=[pl.BlockSpec(memory_space=pltpu.SMEM)] + [vmem] * 5,
        out_specs=(vmem, vmem),
        scratch_shapes=[pltpu.VMEM((4 * tokens, half), jnp.bfloat16)],
        name="dispatch_rows",
    )(core.astype(jnp.int32).reshape(1), ids.T, weight.T, resid, cotangent, gain.reshape(1, -1))


def resid_mixed_kernel(place_ref, normed_ref, cot_ref, resid_ref, gain_ref, *refs):
    blocks, (out_ref, mixed_ref) = refs[:8], refs[8:]
    tokens = resid_ref.shape[0]
    for at in range(0, tokens, 32):
        rows = slice(at, at + 32)
        r = resid_ref[rows, :].astype(jnp.float32)
        inverse_rms = lax.rsqrt(jnp.mean(r * r, axis=1, keepdims=True) + epsilon)
        unit = r * inverse_rms
        scaled = normed_ref[rows, :].astype(jnp.float32) * gain_ref[...]
        mean = jnp.mean(scaled * unit, axis=1, keepdims=True)
        grad = cot_ref[rows, :].astype(jnp.float32) + inverse_rms * (scaled - unit * mean)
        out_ref[rows, :] = grad.astype(jnp.bfloat16)
    depth = blocks[0].shape[0]
    total = jnp.zeros(mixed_ref.shape, jnp.float32)
    for k in range(8):
        at = pl.multiple_of(jnp.bitwise_and(place_ref[0] + (8 - k), 7) * depth, depth)
        total = total + jnp.dot(
            out_ref[:, pl.ds(at, depth)], blocks[k][...], preferred_element_type=jnp.float32
        )
    mixed_ref[...] = total.astype(jnp.bfloat16)


def resid_mixed(place, grad_normed, cotangent, resid, gain, blocks):
    vmem = pl.BlockSpec(memory_space=pltpu.VMEM)
    return pl.pallas_call(
        resid_mixed_kernel,
        out_shape=(
            jax.ShapeDtypeStruct(resid.shape, jnp.bfloat16),
            jax.ShapeDtypeStruct((resid.shape[0], blocks[0].shape[1]), jnp.bfloat16),
        ),
        in_specs=[pl.BlockSpec(memory_space=pltpu.SMEM)] + [vmem] * 12,
        out_specs=(vmem, vmem),
        name="resid_mixed",
    )(
        place.astype(jnp.int32).reshape(1),
        grad_normed,
        cotangent,
        resid,
        gain.reshape(1, -1),
        *blocks,
    )


def on_device_body(
    resid,
    norm_gain,
    cotangent,
    route_ids,
    route_weight,
    expert_gate,
    expert_up,
    expert_down,
    out_proj,
    mixed,
    query,
    key,
    value,
    log_decay,
    span_state,
):
    tokens_here = resid.shape[0]
    model_width = resid.shape[1]
    half = model_width // 2
    sp_count = lax.axis_size(SP)
    y_count = lax.axis_size("y")
    experts = sp_count * expert_gate.shape[0]
    capacity = CAPACITY
    slots = experts * capacity
    core = lax.axis_index("c")
    sent, slot_rows = dispatch_rows(
        core, route_ids, route_weight, resid, cotangent, norm_gain, experts
    )
    slot_a, slot_b = slot_rows[0], slot_rows[1]
    sent = sent.reshape(sp_count, 2 * capacity, half)
    own = lax.all_to_all(sent, SP, 0, 0, tiled=True).reshape(2 * slots, half)
    proj_near, _ = lax.optimization_barrier((out_proj, sent))
    proj_near = lax.all_gather(proj_near, "x", axis=0, tiled=True)
    other = lax.ppermute(own, "c", [(0, 1), (1, 0)])
    rows_in = jnp.where(core == 0, own, other)
    rows_cot = jnp.where(core == 0, other, own)

    gate_w, up_w, down_w = expert_gate[0], expert_up[0], expert_down[0]
    width = gate_w.shape[1]
    into_w = jnp.concatenate([gate_w[:half], gate_w[half:], up_w[:half], up_w[half:]], axis=1)
    down_two = jnp.concatenate([down_w[:, :half], down_w[:, half:]], axis=0)
    pre = jnp.dot(rows_in, into_w, preferred_element_type=jnp.float32)
    gate_pre = pre[:, :width] + jnp.roll(pre[:, width : 2 * width], -1, axis=0)
    up_pre = pre[:, 2 * width : 3 * width] + jnp.roll(pre[:, 3 * width :], -1, axis=0)
    hid = lax.dot_general(
        rows_cot, down_two, (((1,), (1,)), ((), ())), preferred_element_type=jnp.float32
    )
    grad_hidden = hid[:, :width] + jnp.roll(hid[:, width:], -1, axis=0)
    gate_sig = jax.nn.sigmoid(gate_pre)
    first = (lax.broadcasted_iota(jnp.int32, (2 * slots, 1), 0) % 2) == 0

    def kept(values):
        return jnp.where(first, values, 0.0).astype(jnp.bfloat16)

    hidden = kept(gate_pre * gate_sig * up_pre)
    grad_up_act = kept(grad_hidden * gate_pre * gate_sig)
    grad_gate_act = kept(grad_hidden * up_pre * gate_sig * (1.0 + gate_pre * (1.0 - gate_sig)))
    acts = jnp.concatenate([grad_gate_act, grad_up_act], axis=1)
    pick = (
        lax.broadcasted_iota(jnp.int32, (slots, 2 * slots), 1)
        == 2 * lax.broadcasted_iota(jnp.int32, (slots, 2 * slots), 0)
    ).astype(jnp.bfloat16)
    acts = jnp.dot(pick, acts, preferred_element_type=jnp.float32).astype(jnp.bfloat16)
    out_w = jnp.concatenate([gate_w, up_w], axis=1).reshape(y_count, 2, width, 2 * width)
    out_own = jnp.where(core == 0, out_w[:, 0], out_w[:, 1]).reshape(half, 2 * width)
    out_other = jnp.where(core == 0, out_w[:, 1], out_w[:, 0]).reshape(half, 2 * width)

    def onto(weights):
        return lax.dot_general(
            acts, weights, (((1,), (1,)), ((), ())), preferred_element_type=jnp.float32
        )

    passed = lax.ppermute(onto(out_other).astype(jnp.bfloat16), "c", [(0, 1), (1, 0)])
    pair_sum = (onto(out_own) + passed.astype(jnp.float32)).astype(jnp.bfloat16)
    parts = pair_sum.reshape(slots, y_count, width).transpose(1, 0, 2)
    swapped = lax.all_to_all(parts, "y", 0, 0, tiled=True)
    summed = sum_parts(swapped).astype(jnp.bfloat16)
    proj_tied, _ = lax.optimization_barrier((proj_near, parts))
    z_place = lax.axis_index("z")
    blocks = [proj_near] + [None] * 7
    for k in range(1, 8):
        blocks[k] = lax.ppermute(proj_tied, "z", [(i, (i + k) % 8) for i in range(8)])

    def beside(values):
        return jnp.concatenate([values, jnp.roll(values, 1, axis=0)], axis=1)

    grad_in_w = named_dot(
        rows_in, jnp.concatenate([beside(grad_gate_act), beside(grad_up_act)], axis=1)
    )
    grad_gate_w = jnp.concatenate([grad_in_w[:, :width], grad_in_w[:, width : 2 * width]], axis=0)
    grad_up_w = jnp.concatenate(
        [grad_in_w[:, 2 * width : 3 * width], grad_in_w[:, 3 * width :]], axis=0
    )
    grad_out_w = named_dot(beside(hidden), rows_cot)
    grad_down_w = jnp.concatenate([grad_out_w[:width], grad_out_w[width:]], axis=1)

    returned = lax.all_to_all(
        summed.reshape(experts, capacity, -1), SP, split_axis=0, concat_axis=0, tiled=True
    )
    flat_rows = returned.reshape(slots, -1)
    slot_index = lax.broadcasted_iota(jnp.int32, (slots, tokens_here), 0)
    slot_tokens = ((slot_index == slot_a[None, :]) | (slot_index == slot_b[None, :])).astype(
        jnp.bfloat16
    )
    grad_normed = lax.all_gather(
        lax.dot_general(
            slot_tokens, flat_rows, (((0,), (0,)), ((), ())), preferred_element_type=jnp.float32
        ).astype(jnp.bfloat16),
        ("y", "c"),
        axis=1,
        tiled=True,
    )
    grad_resid, grad_mixed = resid_mixed(
        z_place, grad_normed, cotangent, resid, norm_gain, blocks
    )
    share = lax.dot_general(
        grad_resid, mixed, (((0,), (0,)), ((), ())), preferred_element_type=jnp.float32
    ).astype(jnp.bfloat16)
    query_scale = KEY_CHANNELS ** (-0.5)
    query_rows = query.astype(jnp.float32) * query_scale
    key_rows = key.astype(jnp.float32)
    value_rows = value.astype(jnp.float32)
    grad_rows = grad_mixed.astype(jnp.float32)
    kept_terms, summary = span_forward(
        query_rows, key_rows, value_rows, grad_rows, log_decay, span_state[0, 0]
    )
    own_decay, own_state = summary
    near_filled = to_all(with_decay(own_state, own_decay), "x")
    near_states, near_decays = split_decay(near_filled)
    near_sum, near_factor = later_sum(near_states, near_decays, lax.axis_index("x"))
    group_sum, group_factor = later_sum(near_states, near_decays, -1)
    far_filled = to_all(with_decay(group_sum, group_factor), "z")
    far_states, far_decays = split_decay(far_filled)
    z_count, x_count = lax.axis_size("z"), lax.axis_size("x")
    share_rows = model_width // sp_count
    share_x = share.reshape(z_count, x_count, share_rows, -1).transpose(1, 0, 2, 3)
    place = lax.axis_index("x")

    def for_place(k):
        at = jnp.bitwise_and(place + k, x_count - 1).astype(jnp.uint32)
        return lax.dynamic_index_in_dim(share_x, at, 0, keepdims=False)

    share_sum = for_place(0).astype(jnp.float32)
    for k in range(1, 4):
        passed = lax.ppermute(
            for_place(k), "x", [(i, (i + k) % 4) for i in range(4)]
        )
        share_sum = share_sum + passed.astype(jnp.float32)
    share_z = share_sum.astype(jnp.bfloat16)
    share_z = lax.all_to_all(share_z, "z", 0, 0, tiled=True)
    grad_out_proj = sum_parts(share_z)
    far_sum, _ = later_sum(far_states, far_decays, lax.axis_index("z"))
    exit_cot = near_sum + near_factor[:, None] * far_sum
    grad_query, grad_key, grad_value, grad_log_decay = span_backward(
        query_rows, key_rows, value_rows, grad_rows, kept_terms, exit_cot
    )
    grad_query = (grad_query * query_scale).astype(jnp.bfloat16)
    grad_key = grad_key.astype(jnp.bfloat16)
    grad_value = grad_value.astype(jnp.bfloat16)
    return (
        grad_gate_w[None],
        grad_up_w[None],
        grad_down_w[None],
        grad_out_proj,
        grad_query,
        grad_key,
        grad_value,
        grad_log_decay,
    )


def solution(mesh):
    finer = Mesh(mesh.devices.reshape(8, 4, 8, 2), ("z", "x", "y", "c"))
    in_specs = (
        P(SP, None),
        P(),
        P(SP, None),
        P(SP, None),
        P(SP, None),
        P(SP, None, TP),
        P(SP, None, TP),
        P(SP, TP, None),
        P(SP, TP),
        P(SP, TP),
        P(SP, TP),
        P(SP, TP),
        P(SP, TP),
        P(SP, TP),
        P(SP, TP, None, None),
    )
    out_specs = (
        P(SP, None, TP),
        P(SP, None, TP),
        P(SP, TP, None),
        P(SP, TP),
        P(SP, TP),
        P(SP, TP),
        P(SP, TP),
        P(SP, TP),
    )
    return jax.shard_map(
        on_device_body, mesh=finer, in_specs=in_specs, out_specs=out_specs, check_vma=False
    )
```

```python
import jax
import jax.numpy as jnp
from jax import lax
from jax.experimental import pallas as pl
from jax.experimental.pallas import tpu as pltpu
from jax.sharding import Mesh
from jax.sharding import PartitionSpec as P


KEY_CHANNELS = 128
DV = 256
CAPACITY = 12
BLOCK = 64
SP = ("z", "x")
TP = ("y", "c")


epsilon = 1e-06


def sum_parts(tiles):
    return jnp.sum(tiles.astype(jnp.float32), axis=0)


def later_sum(states, decays, place):
    count = states.shape[0]
    total = jnp.zeros(states.shape[1:], jnp.float32)
    factor = jnp.ones(decays.shape[1:], jnp.float32)
    for k in range(count):
        later = k > place
        total = total + jnp.where(later, factor, 0.0)[:, None] * states[k].astype(jnp.float32)
        factor = jnp.where(later, factor * decays[k], factor)
    return total, factor


def named_dot(left, right):
    return lax.dot_general(
        left, right, (((0,), (0,)), ((), ())), preferred_element_type=jnp.float32
    ).astype(jnp.bfloat16)


def to_all(array, axis):
    count = lax.axis_size(axis)
    copies = jnp.broadcast_to(array[None], (count, *array.shape))
    return lax.all_to_all(copies, axis, 0, 0, tiled=True)


def with_decay(state, decay):
    row = jnp.pad(decay[None, :], ((0, 7), (0, DV - KEY_CHANNELS)))
    return jnp.concatenate([state, row], axis=0).astype(jnp.bfloat16)


def split_decay(filled):
    decays = filled[:, KEY_CHANNELS, :KEY_CHANNELS].astype(jnp.float32)
    return filled[:, :KEY_CHANNELS], decays


def into_blocks(values):
    return values.reshape(values.shape[0] // BLOCK, BLOCK, values.shape[1])


def span_forward(query_rows, key_rows, value_rows, grad_rows, decay_rows, entry_state):
    query_blk = into_blocks(query_rows)
    key_blk = into_blocks(key_rows)
    value_blk = into_blocks(value_rows)
    grad_blk = into_blocks(grad_rows)
    cumlog = jnp.cumsum(into_blocks(decay_rows), axis=1)
    block_total = cumlog[:, -1, :]
    to_end = jnp.exp(block_total[:, None, :] - cumlog)
    inner_part = jnp.einsum("nsd,nsj->ndj", key_blk * to_end, value_blk)

    def forward_step(carry_state, step_item):
        piece_part, block_sum = step_item
        return (jnp.exp(block_sum)[:, None] * carry_state + piece_part, carry_state)

    end_state, starts = lax.scan(
        forward_step, entry_state, (inner_part, block_total), unroll=True
    )
    own_part = jnp.einsum("ntd,ntj->ndj", query_blk * jnp.exp(cumlog), grad_blk)

    def backward_step(carry_state, step_item):
        piece_part, block_sum = step_item
        return (jnp.exp(block_sum)[:, None] * carry_state + piece_part, carry_state)

    start_cot, after_cot = lax.scan(
        backward_step,
        jnp.zeros_like(entry_state),
        (own_part, block_total),
        reverse=True,
        unroll=True,
    )
    span_total = jnp.sum(block_total, axis=0)
    later_log = span_total[None, :] - jnp.cumsum(block_total, axis=0)
    return ((cumlog, starts, after_cot, later_log, end_state), (jnp.exp(span_total), start_cot))


def span_backward(query_rows, key_rows, value_rows, grad_rows, kept_terms, exit_cot):
    cumlog, starts, after_cot, later_log, end_state = kept_terms
    query_blk = into_blocks(query_rows)
    key_blk = into_blocks(key_rows)
    value_blk = into_blocks(value_rows)
    grad_blk = into_blocks(grad_rows)
    exit_cots = after_cot + jnp.exp(later_log)[:, :, None] * exit_cot
    causal = jnp.arange(BLOCK)[:, None] >= jnp.arange(BLOCK)[None, :]
    decays = jnp.exp(
        jnp.where(causal[None, :, :, None], cumlog[:, :, None, :] - cumlog[:, None, :, :], -jnp.inf)
    )
    scores = jnp.einsum("ntd,nsd,ntsd->nts", query_blk, key_blk, decays)
    grad_scores = jnp.einsum("ntj,nsj->nts", grad_blk, value_blk)
    grad_query = jnp.exp(cumlog) * jnp.einsum("ntj,ndj->ntd", grad_blk, starts)
    grad_query = grad_query + jnp.einsum("nts,nsd,ntsd->ntd", grad_scores, key_blk, decays)
    to_end = jnp.exp(cumlog[:, -1:, :] - cumlog)
    grad_key = jnp.einsum("nts,ntd,ntsd->nsd", grad_scores, query_blk, decays)
    grad_key = grad_key + to_end * jnp.einsum("nsj,ndj->nsd", value_blk, exit_cots)
    grad_value = jnp.einsum("nts,ntj->nsj", scores, grad_blk)
    grad_value = grad_value + jnp.einsum("nsd,ndj->nsj", key_blk * to_end, exit_cots)
    length = query_rows.shape[0]
    key_width = query_rows.shape[1]
    per_position = (query_blk * grad_query - key_blk * grad_key).reshape(length, key_width)
    grad_log = (
        jnp.flip(jnp.cumsum(jnp.flip(per_position, 0), 0), 0)
        + jnp.sum(end_state * exit_cot, axis=1)[None, :]
    )
    return (
        grad_query.reshape(length, key_width),
        grad_key.reshape(length, key_width),
        grad_value.reshape(length, value_rows.shape[1]),
        grad_log,
    )


def dispatch_rows_kernel(core_ref, ids_ref, weight_ref, resid_ref, cot_ref, gain_ref, sent_ref, slot_ref, rows_ref):
    tokens, model_width = resid_ref.shape
    half = model_width // 2
    experts = sent_ref.shape[0] // (2 * CAPACITY)

    square = (tokens, tokens)
    row_at = lax.broadcasted_iota(jnp.int32, square, 0)
    col_at = lax.broadcasted_iota(jnp.int32, square, 1)
    along = [ids_ref[k : k + 1, :].astype(jnp.float32) for k in range(2)]

    @pl.when(core_ref[0] == 0)
    def _():
        for at in range(0, tokens, 32):
            r = resid_ref[at : at + 32, :].astype(jnp.float32)
            inverse_rms = lax.rsqrt(jnp.mean(r * r, axis=1, keepdims=True) + epsilon)
            normed = (r * inverse_rms * gain_ref[...]).astype(jnp.bfloat16)
            for k in range(2):
                for h in range(2):
                    low = (2 * k + h) * tokens + at
                    rows_ref[low : low + 32, :] = normed[:, h * half : (h + 1) * half]

    @pl.when(core_ref[0] != 0)
    def _():
        weights = []
        for k in range(2):
            spread = jnp.broadcast_to(weight_ref[k : k + 1, :], square)
            weights.append(
                jnp.sum(jnp.where(row_at == col_at, spread, 0.0), axis=1, keepdims=True)
            )
        for at in range(0, tokens, 32):
            c = cot_ref[at : at + 32, :].astype(jnp.float32)
            for k in range(2):
                sent = (c * weights[k][at : at + 32, :]).astype(jnp.bfloat16)
                for h in range(2):
                    low = (2 * k + h) * tokens + at
                    rows_ref[low : low + 32, :] = sent[:, h * half : (h + 1) * half]

    expert_at = lax.broadcasted_iota(jnp.int32, (experts, tokens), 0).astype(jnp.float32)
    named = [(expert_at == a).astype(jnp.float32) for a in along]
    earlier = (row_at < col_at).astype(jnp.bfloat16)
    before = jnp.dot(
        (named[0] + named[1]).astype(jnp.bfloat16), earlier, preferred_element_type=jnp.float32
    )
    slots = [
        (a * CAPACITY + jnp.sum(n * before, axis=0, keepdims=True)).astype(jnp.int32)
        for a, n in zip(along, named)
    ]
    slot_ref[...] = jnp.concatenate(slots + [jnp.zeros((6, tokens), jnp.int32)], axis=0)
    step = 256
    for at in range(0, sent_ref.shape[0], step):
        packed = lax.broadcasted_iota(jnp.int32, (step, tokens), 0) + at
        hits = [
            jnp.where(packed == 2 * slot + h, 1.0, 0.0).astype(jnp.bfloat16)
            for slot in slots
            for h in range(2)
        ]
        sent_ref[at : at + step, :] = jnp.dot(
            jnp.concatenate(hits, axis=1), rows_ref[...], preferred_element_type=jnp.float32
        ).astype(jnp.bfloat16)


def dispatch_rows(core, ids, weight, resid, cotangent, gain, experts):
    tokens, model_width = resid.shape
    half = model_width // 2
    vmem = pl.BlockSpec(memory_space=pltpu.VMEM)
    return pl.pallas_call(
        dispatch_rows_kernel,
        out_shape=(
            jax.ShapeDtypeStruct((2 * experts * CAPACITY, half), jnp.bfloat16),
            jax.ShapeDtypeStruct((8, tokens), jnp.int32),
        ),
        in_specs=[pl.BlockSpec(memory_space=pltpu.SMEM)] + [vmem] * 5,
        out_specs=(vmem, vmem),
        scratch_shapes=[pltpu.VMEM((4 * tokens, half), jnp.bfloat16)],
        name="dispatch_rows",
    )(core.astype(jnp.int32).reshape(1), ids.T, weight.T, resid, cotangent, gain.reshape(1, -1))


def pair_tiles_kernel(own_ref, passed_ref, out_ref):
    width = out_ref.shape[2]
    for k in range(out_ref.shape[0]):
        cols = slice(k * width, (k + 1) * width)
        total = own_ref[:, cols] + passed_ref[:, cols].astype(jnp.float32)
        out_ref[k] = total.astype(jnp.bfloat16)


def pair_tiles(own, passed, count):
    rows, width = own.shape
    vmem = pl.BlockSpec(memory_space=pltpu.VMEM)
    return pl.pallas_call(
        pair_tiles_kernel,
        out_shape=jax.ShapeDtypeStruct((count, rows, width // count), jnp.bfloat16),
        in_specs=[vmem, vmem],
        out_specs=vmem,
        name="pair_tiles",
    )(own, passed)


def resid_mixed_kernel(place_ref, normed_ref, cot_ref, resid_ref, gain_ref, *refs):
    blocks, (out_ref, mixed_ref) = refs[:8], refs[8:]
    tokens = resid_ref.shape[0]
    for at in range(0, tokens, 32):
        rows = slice(at, at + 32)
        r = resid_ref[rows, :].astype(jnp.float32)
        inverse_rms = lax.rsqrt(jnp.mean(r * r, axis=1, keepdims=True) + epsilon)
        unit = r * inverse_rms
        scaled = normed_ref[rows, :].astype(jnp.float32) * gain_ref[...]
        mean = jnp.mean(scaled * unit, axis=1, keepdims=True)
        grad = cot_ref[rows, :].astype(jnp.float32) + inverse_rms * (scaled - unit * mean)
        out_ref[rows, :] = grad.astype(jnp.bfloat16)
    depth = blocks[0].shape[0]
    total = jnp.zeros(mixed_ref.shape, jnp.float32)
    for k in range(8):
        at = pl.multiple_of(jnp.bitwise_and(place_ref[0] + (8 - k), 7) * depth, depth)
        total = total + jnp.dot(
            out_ref[:, pl.ds(at, depth)], blocks[k][...], preferred_element_type=jnp.float32
        )
    mixed_ref[...] = total.astype(jnp.bfloat16)


def resid_mixed(place, grad_normed, cotangent, resid, gain, blocks):
    vmem = pl.BlockSpec(memory_space=pltpu.VMEM)
    return pl.pallas_call(
        resid_mixed_kernel,
        out_shape=(
            jax.ShapeDtypeStruct(resid.shape, jnp.bfloat16),
            jax.ShapeDtypeStruct((resid.shape[0], blocks[0].shape[1]), jnp.bfloat16),
        ),
        in_specs=[pl.BlockSpec(memory_space=pltpu.SMEM)] + [vmem] * 12,
        out_specs=(vmem, vmem),
        name="resid_mixed",
    )(
        place.astype(jnp.int32).reshape(1),
        grad_normed,
        cotangent,
        resid,
        gain.reshape(1, -1),
        *blocks,
    )


def on_device_body(
    resid,
    norm_gain,
    cotangent,
    route_ids,
    route_weight,
    expert_gate,
    expert_up,
    expert_down,
    out_proj,
    mixed,
    query,
    key,
    value,
    log_decay,
    span_state,
):
    tokens_here = resid.shape[0]
    model_width = resid.shape[1]
    half = model_width // 2
    sp_count = lax.axis_size(SP)
    y_count = lax.axis_size("y")
    experts = sp_count * expert_gate.shape[0]
    capacity = CAPACITY
    slots = experts * capacity
    core = lax.axis_index("c")
    sent, slot_rows = dispatch_rows(
        core, route_ids, route_weight, resid, cotangent, norm_gain, experts
    )
    slot_a, slot_b = slot_rows[0], slot_rows[1]
    sent = sent.reshape(sp_count, 2 * capacity, half)
    gate_w, up_w, down_w = expert_gate[0], expert_up[0], expert_down[0]
    width = gate_w.shape[1]
    own = lax.all_to_all(sent, SP, 0, 0, tiled=True).reshape(2 * slots, half)
    proj_near, _ = lax.optimization_barrier((out_proj, sent))
    proj_near = lax.all_gather(proj_near, "x", axis=0, tiled=True)
    other = lax.ppermute(own, "c", [(0, 1), (1, 0)])
    rows_in = jnp.where(core == 0, own, other)
    rows_cot = jnp.where(core == 0, other, own)

    into_w = jnp.concatenate([gate_w[:half], gate_w[half:], up_w[:half], up_w[half:]], axis=1)
    down_t = jnp.transpose(down_w)
    down_t = jnp.concatenate([down_t[:half], down_t[half:]], axis=1)
    down_t = jnp.pad(down_t, ((0, 0), (0, 2 * width)))
    own_w = jnp.where(core == 0, into_w, down_t)
    other_w = jnp.where(core == 0, down_t, into_w)
    own_w, other_w = lax.optimization_barrier((own_w, other_w))
    own_pre = jnp.dot(own, own_w, preferred_element_type=jnp.float32)
    own_pre = lax.optimization_barrier(own_pre)
    other_pre = jnp.dot(other, other_w, preferred_element_type=jnp.float32)
    pre = jnp.where(core == 0, own_pre, other_pre)
    hid = jnp.where(core == 0, other_pre[:, : 2 * width], own_pre[:, : 2 * width])
    gate_pre = pre[:, :width] + jnp.roll(pre[:, width : 2 * width], -1, axis=0)
    up_pre = pre[:, 2 * width : 3 * width] + jnp.roll(pre[:, 3 * width :], -1, axis=0)
    grad_hidden = hid[:, :width] + jnp.roll(hid[:, width:], -1, axis=0)
    gate_sig = jax.nn.sigmoid(gate_pre)
    first = (lax.broadcasted_iota(jnp.int32, (2 * slots, 1), 0) % 2) == 0

    def kept(values):
        return jnp.where(first, values, 0.0).astype(jnp.bfloat16)

    hidden = kept(gate_pre * gate_sig * up_pre)
    grad_up_act = kept(grad_hidden * gate_pre * gate_sig)
    grad_gate_act = kept(grad_hidden * up_pre * gate_sig * (1.0 + gate_pre * (1.0 - gate_sig)))
    acts = jnp.concatenate([grad_gate_act, grad_up_act], axis=1)
    pick = (
        lax.broadcasted_iota(jnp.int32, (slots, 2 * slots), 1)
        == 2 * lax.broadcasted_iota(jnp.int32, (slots, 2 * slots), 0)
    ).astype(jnp.bfloat16)
    acts = jnp.dot(pick, acts, preferred_element_type=jnp.float32).astype(jnp.bfloat16)
    out_w = jnp.concatenate([gate_w, up_w], axis=1).reshape(y_count, 2, width, 2 * width)
    out_own = jnp.where(core == 0, out_w[:, 0], out_w[:, 1]).reshape(half, 2 * width)
    out_other = jnp.where(core == 0, out_w[:, 1], out_w[:, 0]).reshape(half, 2 * width)

    def onto(weights):
        return lax.dot_general(
            acts, weights, (((1,), (1,)), ((), ())), preferred_element_type=jnp.float32
        )

    passed = lax.ppermute(onto(out_other).astype(jnp.bfloat16), "c", [(0, 1), (1, 0)])
    own_parts = onto(out_own)
    parts = pair_tiles(own_parts, passed, y_count)
    swapped = lax.all_to_all(parts, "y", 0, 0, tiled=True)
    summed = sum_parts(swapped).astype(jnp.bfloat16)
    proj_tied, _ = lax.optimization_barrier((proj_near, parts))
    proj_early, _ = lax.optimization_barrier((proj_near, own))
    proj_mid, _ = lax.optimization_barrier((proj_near, acts))
    z_place = lax.axis_index("z")
    blocks = [proj_near] + [None] * 7
    for k in range(1, 8):
        sent_block = proj_early if k == 5 else proj_mid if k == 4 else proj_tied
        blocks[k] = lax.ppermute(sent_block, "z", [(i, (i + k) % 8) for i in range(8)])

    def beside(values):
        return jnp.concatenate([values, jnp.roll(values, 1, axis=0)], axis=1)

    grad_in_w = named_dot(
        rows_in, jnp.concatenate([beside(grad_gate_act), beside(grad_up_act)], axis=1)
    )
    grad_gate_w = jnp.concatenate([grad_in_w[:, :width], grad_in_w[:, width : 2 * width]], axis=0)
    grad_up_w = jnp.concatenate(
        [grad_in_w[:, 2 * width : 3 * width], grad_in_w[:, 3 * width :]], axis=0
    )
    grad_out_w = named_dot(beside(hidden), rows_cot)
    grad_down_w = jnp.concatenate([grad_out_w[:width], grad_out_w[width:]], axis=1)

    returned = lax.all_to_all(
        summed.reshape(experts, capacity, -1), SP, split_axis=0, concat_axis=0, tiled=True
    )
    flat_rows = returned.reshape(slots, -1)
    slot_index = lax.broadcasted_iota(jnp.int32, (slots, tokens_here), 0)
    slot_tokens = ((slot_index == slot_a[None, :]) | (slot_index == slot_b[None, :])).astype(
        jnp.bfloat16
    )
    grad_normed = lax.all_gather(
        lax.dot_general(
            slot_tokens, flat_rows, (((0,), (0,)), ((), ())), preferred_element_type=jnp.float32
        ).astype(jnp.bfloat16),
        ("y", "c"),
        axis=1,
        tiled=True,
    )
    grad_resid, grad_mixed = resid_mixed(
        z_place, grad_normed, cotangent, resid, norm_gain, blocks
    )
    share = lax.dot_general(
        grad_resid, mixed, (((0,), (0,)), ((), ())), preferred_element_type=jnp.float32
    ).astype(jnp.bfloat16)
    query_scale = KEY_CHANNELS ** (-0.5)
    query_rows = query.astype(jnp.float32) * query_scale
    key_rows = key.astype(jnp.float32)
    value_rows = value.astype(jnp.float32)
    grad_rows = grad_mixed.astype(jnp.float32)
    kept_terms, summary = span_forward(
        query_rows, key_rows, value_rows, grad_rows, log_decay, span_state[0, 0]
    )
    own_decay, own_state = summary
    near_filled = to_all(with_decay(own_state, own_decay), "x")
    near_states, near_decays = split_decay(near_filled)
    near_sum, near_factor = later_sum(near_states, near_decays, lax.axis_index("x"))
    group_sum, group_factor = later_sum(near_states, near_decays, -1)
    far_filled = to_all(with_decay(group_sum, group_factor), "z")
    far_states, far_decays = split_decay(far_filled)
    z_count, x_count = lax.axis_size("z"), lax.axis_size("x")
    share_rows = model_width // sp_count
    share_x = share.reshape(z_count, x_count, share_rows, -1).transpose(1, 0, 2, 3)
    place = lax.axis_index("x")

    def for_place(k):
        at = jnp.bitwise_and(place + k, x_count - 1).astype(jnp.uint32)
        return lax.dynamic_index_in_dim(share_x, at, 0, keepdims=False)

    share_sum = for_place(0).astype(jnp.float32)
    for k in range(1, 4):
        passed = lax.ppermute(
            for_place(k), "x", [(i, (i + k) % 4) for i in range(4)]
        )
        share_sum = share_sum + passed.astype(jnp.float32)
    share_z = share_sum.astype(jnp.bfloat16)
    share_z = lax.all_to_all(share_z, "z", 0, 0, tiled=True)
    grad_out_proj = sum_parts(share_z)
    far_sum, _ = later_sum(far_states, far_decays, lax.axis_index("z"))
    exit_cot = near_sum + near_factor[:, None] * far_sum
    grad_query, grad_key, grad_value, grad_log_decay = span_backward(
        query_rows, key_rows, value_rows, grad_rows, kept_terms, exit_cot
    )
    grad_query = (grad_query * query_scale).astype(jnp.bfloat16)
    grad_key = grad_key.astype(jnp.bfloat16)
    grad_value = grad_value.astype(jnp.bfloat16)
    return (
        grad_gate_w[None],
        grad_up_w[None],
        grad_down_w[None],
        grad_out_proj,
        grad_query,
        grad_key,
        grad_value,
        grad_log_decay,
    )


def solution(mesh):
    finer = Mesh(mesh.devices.reshape(8, 4, 8, 2), ("z", "x", "y", "c"))
    in_specs = (
        P(SP, None),
        P(),
        P(SP, None),
        P(SP, None),
        P(SP, None),
        P(SP, None, TP),
        P(SP, None, TP),
        P(SP, TP, None),
        P(SP, TP),
        P(SP, TP),
        P(SP, TP),
        P(SP, TP),
        P(SP, TP),
        P(SP, TP),
        P(SP, TP, None, None),
    )
    out_specs = (
        P(SP, None, TP),
        P(SP, None, TP),
        P(SP, TP, None),
        P(SP, TP),
        P(SP, TP),
        P(SP, TP),
        P(SP, TP),
        P(SP, TP),
    )
    return jax.shard_map(
        on_device_body, mesh=finer, in_specs=in_specs, out_specs=out_specs, check_vma=False
    )
```

```python
import jax
import jax.numpy as jnp
from jax import lax
from jax.experimental import pallas as pl
from jax.experimental.pallas import tpu as pltpu
from jax.sharding import Mesh
from jax.sharding import PartitionSpec as P


KEY_CHANNELS = 128
DV = 256
CAPACITY = 12
BLOCK = 64
SP = ("z", "x")
TP = ("y", "c")


epsilon = 1e-06


def sum_parts(tiles):
    return jnp.sum(tiles.astype(jnp.float32), axis=0)


def later_sum(states, decays, place):
    count = states.shape[0]
    total = jnp.zeros(states.shape[1:], jnp.float32)
    factor = jnp.ones(decays.shape[1:], jnp.float32)
    for k in range(count):
        later = k > place
        total = total + jnp.where(later, factor, 0.0)[:, None] * states[k].astype(jnp.float32)
        factor = jnp.where(later, factor * decays[k], factor)
    return total, factor


def named_dot(left, right):
    return lax.dot_general(
        left, right, (((0,), (0,)), ((), ())), preferred_element_type=jnp.float32
    ).astype(jnp.bfloat16)


def to_all(array, axis):
    count = lax.axis_size(axis)
    copies = jnp.broadcast_to(array[None], (count, *array.shape))
    return lax.all_to_all(copies, axis, 0, 0, tiled=True)


def with_decay(state, decay):
    row = jnp.pad(decay[None, :], ((0, 7), (0, DV - KEY_CHANNELS)))
    return jnp.concatenate([state, row], axis=0).astype(jnp.bfloat16)


def split_decay(filled):
    decays = filled[:, KEY_CHANNELS, :KEY_CHANNELS].astype(jnp.float32)
    return filled[:, :KEY_CHANNELS], decays


def into_blocks(values):
    return values.reshape(values.shape[0] // BLOCK, BLOCK, values.shape[1])


def span_forward(query_rows, key_rows, value_rows, grad_rows, decay_rows, entry_state):
    query_blk = into_blocks(query_rows)
    key_blk = into_blocks(key_rows)
    value_blk = into_blocks(value_rows)
    grad_blk = into_blocks(grad_rows)
    cumlog = jnp.cumsum(into_blocks(decay_rows), axis=1)
    block_total = cumlog[:, -1, :]
    to_end = jnp.exp(block_total[:, None, :] - cumlog)
    inner_part = jnp.einsum("nsd,nsj->ndj", key_blk * to_end, value_blk)

    def forward_step(carry_state, step_item):
        piece_part, block_sum = step_item
        return (jnp.exp(block_sum)[:, None] * carry_state + piece_part, carry_state)

    end_state, starts = lax.scan(
        forward_step, entry_state, (inner_part, block_total), unroll=True
    )
    second_part = jnp.einsum("td,tj->dj", query_blk[1] * jnp.exp(cumlog[1]), grad_blk[1])
    after_cot = jnp.stack([second_part, jnp.zeros_like(second_part)])
    span_total = jnp.sum(block_total, axis=0)
    later_log = span_total[None, :] - jnp.cumsum(block_total, axis=0)
    return (cumlog, starts, after_cot, later_log, end_state)


def span_backward(query_rows, key_rows, value_rows, grad_rows, kept_terms, exit_cot):
    cumlog, starts, after_cot, later_log, end_state = kept_terms
    query_blk = into_blocks(query_rows)
    key_blk = into_blocks(key_rows)
    value_blk = into_blocks(value_rows)
    grad_blk = into_blocks(grad_rows)
    exit_cots = after_cot + jnp.exp(later_log)[:, :, None] * exit_cot
    causal = jnp.arange(BLOCK)[:, None] >= jnp.arange(BLOCK)[None, :]
    decays = jnp.exp(
        jnp.where(causal[None, :, :, None], cumlog[:, :, None, :] - cumlog[:, None, :, :], -jnp.inf)
    )
    scores = jnp.einsum("ntd,nsd,ntsd->nts", query_blk, key_blk, decays)
    grad_scores = jnp.einsum("ntj,nsj->nts", grad_blk, value_blk)
    grad_query = jnp.exp(cumlog) * jnp.einsum("ntj,ndj->ntd", grad_blk, starts)
    grad_query = grad_query + jnp.einsum("nts,nsd,ntsd->ntd", grad_scores, key_blk, decays)
    to_end = jnp.exp(cumlog[:, -1:, :] - cumlog)
    grad_key = jnp.einsum("nts,ntd,ntsd->nsd", grad_scores, query_blk, decays)
    grad_key = grad_key + to_end * jnp.einsum("nsj,ndj->nsd", value_blk, exit_cots)
    grad_value = jnp.einsum("nts,ntj->nsj", scores, grad_blk)
    grad_value = grad_value + jnp.einsum("nsd,ndj->nsj", key_blk * to_end, exit_cots)
    length = query_rows.shape[0]
    key_width = query_rows.shape[1]
    per_position = (query_blk * grad_query - key_blk * grad_key).reshape(length, key_width)
    grad_log = (
        jnp.flip(jnp.cumsum(jnp.flip(per_position, 0), 0), 0)
        + jnp.sum(end_state * exit_cot, axis=1)[None, :]
    )
    return (
        grad_query.reshape(length, key_width),
        grad_key.reshape(length, key_width),
        grad_value.reshape(length, value_rows.shape[1]),
        grad_log,
    )


def dispatch_rows_kernel(core_ref, ids_ref, weight_ref, resid_ref, cot_ref, gain_ref, sent_ref, slot_ref, rows_ref):
    tokens, model_width = resid_ref.shape
    half = model_width // 2
    experts = sent_ref.shape[0] // (2 * CAPACITY)

    square = (tokens, tokens)
    row_at = lax.broadcasted_iota(jnp.int32, square, 0)
    col_at = lax.broadcasted_iota(jnp.int32, square, 1)
    along = [ids_ref[k : k + 1, :].astype(jnp.float32) for k in range(2)]

    @pl.when(core_ref[0] == 0)
    def _():
        for at in range(0, tokens, 32):
            r = resid_ref[at : at + 32, :].astype(jnp.float32)
            inverse_rms = lax.rsqrt(jnp.mean(r * r, axis=1, keepdims=True) + epsilon)
            normed = (r * inverse_rms * gain_ref[...]).astype(jnp.bfloat16)
            for k in range(2):
                for h in range(2):
                    low = (2 * k + h) * tokens + at
                    rows_ref[low : low + 32, :] = normed[:, h * half : (h + 1) * half]

    @pl.when(core_ref[0] != 0)
    def _():
        weights = []
        for k in range(2):
            spread = jnp.broadcast_to(weight_ref[k : k + 1, :], square)
            weights.append(
                jnp.sum(jnp.where(row_at == col_at, spread, 0.0), axis=1, keepdims=True)
            )
        for at in range(0, tokens, 32):
            c = cot_ref[at : at + 32, :].astype(jnp.float32)
            for k in range(2):
                sent = (c * weights[k][at : at + 32, :]).astype(jnp.bfloat16)
                for h in range(2):
                    low = (2 * k + h) * tokens + at
                    rows_ref[low : low + 32, :] = sent[:, h * half : (h + 1) * half]

    expert_at = lax.broadcasted_iota(jnp.int32, (experts, tokens), 0).astype(jnp.float32)
    named = [(expert_at == a).astype(jnp.float32) for a in along]
    earlier = (row_at < col_at).astype(jnp.bfloat16)
    before = jnp.dot(
        (named[0] + named[1]).astype(jnp.bfloat16), earlier, preferred_element_type=jnp.float32
    )
    slots = [
        (a * CAPACITY + jnp.sum(n * before, axis=0, keepdims=True)).astype(jnp.int32)
        for a, n in zip(along, named)
    ]
    slot_ref[...] = jnp.concatenate(slots + [jnp.zeros((6, tokens), jnp.int32)], axis=0)
    step = 256
    for at in range(0, sent_ref.shape[0], step):
        packed = lax.broadcasted_iota(jnp.int32, (step, tokens), 0) + at
        hits = [
            jnp.where(packed == 2 * slot + h, 1.0, 0.0).astype(jnp.bfloat16)
            for slot in slots
            for h in range(2)
        ]
        sent_ref[at : at + step, :] = jnp.dot(
            jnp.concatenate(hits, axis=1), rows_ref[...], preferred_element_type=jnp.float32
        ).astype(jnp.bfloat16)


def dispatch_rows(core, ids, weight, resid, cotangent, gain, experts):
    tokens, model_width = resid.shape
    half = model_width // 2
    vmem = pl.BlockSpec(memory_space=pltpu.VMEM)
    return pl.pallas_call(
        dispatch_rows_kernel,
        out_shape=(
            jax.ShapeDtypeStruct((2 * experts * CAPACITY, half), jnp.bfloat16),
            jax.ShapeDtypeStruct((8, tokens), jnp.int32),
        ),
        in_specs=[pl.BlockSpec(memory_space=pltpu.SMEM)] + [vmem] * 5,
        out_specs=(vmem, vmem),
        scratch_shapes=[pltpu.VMEM((4 * tokens, half), jnp.bfloat16)],
        name="dispatch_rows",
    )(core.astype(jnp.int32).reshape(1), ids.T, weight.T, resid, cotangent, gain.reshape(1, -1))


def resid_mixed_kernel(
    place_ref, normed_ref, cot_ref, resid_ref, gain_ref, query_ref, decay_ref, *refs
):
    blocks, (out_ref, mixed_ref, near_ref) = refs[:8], refs[8:]
    tokens = resid_ref.shape[0]
    for at in range(0, tokens, 32):
        rows = slice(at, at + 32)
        r = resid_ref[rows, :].astype(jnp.float32)
        inverse_rms = lax.rsqrt(jnp.mean(r * r, axis=1, keepdims=True) + epsilon)
        unit = r * inverse_rms
        scaled = normed_ref[rows, :].astype(jnp.float32) * gain_ref[...]
        mean = jnp.mean(scaled * unit, axis=1, keepdims=True)
        grad = cot_ref[rows, :].astype(jnp.float32) + inverse_rms * (scaled - unit * mean)
        out_ref[rows, :] = grad.astype(jnp.bfloat16)
    depth = blocks[0].shape[0]
    total = jnp.zeros(mixed_ref.shape, jnp.float32)
    for k in range(8):
        at = pl.multiple_of(jnp.bitwise_and(place_ref[0] + (8 - k), 7) * depth, depth)
        total = total + jnp.dot(
            out_ref[:, pl.ds(at, depth)], blocks[k][...], preferred_element_type=jnp.float32
        )
    mixed = total.astype(jnp.bfloat16)
    mixed_ref[...] = mixed
    state = jnp.dot(query_ref[...], mixed, preferred_element_type=jnp.float32)
    keys = state.shape[0]
    for k in range(near_ref.shape[0]):
        near_ref[k, :keys, :] = state.astype(jnp.bfloat16)
        near_ref[k, keys:, :] = decay_ref[...].astype(jnp.bfloat16)


def resid_mixed(place, grad_normed, cotangent, resid, gain, blocks, query_cols, decay_row, copies):
    vmem = pl.BlockSpec(memory_space=pltpu.VMEM)
    return pl.pallas_call(
        resid_mixed_kernel,
        out_shape=(
            jax.ShapeDtypeStruct(resid.shape, jnp.bfloat16),
            jax.ShapeDtypeStruct((resid.shape[0], blocks[0].shape[1]), jnp.bfloat16),
            jax.ShapeDtypeStruct(
                (copies, query_cols.shape[0] + decay_row.shape[0], blocks[0].shape[1]), jnp.bfloat16
            ),
        ),
        in_specs=[pl.BlockSpec(memory_space=pltpu.SMEM)] + [vmem] * 14,
        out_specs=(vmem, vmem, vmem),
        name="resid_mixed",
    )(
        place.astype(jnp.int32).reshape(1),
        grad_normed,
        cotangent,
        resid,
        gain.reshape(1, -1),
        query_cols,
        decay_row,
        *blocks,
    )


def on_device_body(
    resid,
    norm_gain,
    cotangent,
    route_ids,
    route_weight,
    expert_gate,
    expert_up,
    expert_down,
    out_proj,
    mixed,
    query,
    key,
    value,
    log_decay,
    span_state,
):
    tokens_here = resid.shape[0]
    model_width = resid.shape[1]
    half = model_width // 2
    sp_count = lax.axis_size(SP)
    y_count = lax.axis_size("y")
    experts = sp_count * expert_gate.shape[0]
    capacity = CAPACITY
    slots = experts * capacity
    core = lax.axis_index("c")
    sent, slot_rows = dispatch_rows(
        core, route_ids, route_weight, resid, cotangent, norm_gain, experts
    )
    slot_a, slot_b = slot_rows[0], slot_rows[1]
    sent = sent.reshape(sp_count, 2 * capacity, half)
    gate_w, up_w, down_w = expert_gate[0], expert_up[0], expert_down[0]
    width = gate_w.shape[1]
    own = lax.all_to_all(sent, SP, 0, 0, tiled=True).reshape(2 * slots, half)
    proj_near, _ = lax.optimization_barrier((out_proj, sent))
    proj_near = lax.all_gather(proj_near, "x", axis=0, tiled=True)
    other = lax.ppermute(own, "c", [(0, 1), (1, 0)])
    rows_in = jnp.where(core == 0, own, other)
    rows_cot = jnp.where(core == 0, other, own)

    into_w = jnp.concatenate([gate_w[:half], gate_w[half:], up_w[:half], up_w[half:]], axis=1)
    down_t = jnp.transpose(down_w)
    down_t = jnp.concatenate([down_t[:half], down_t[half:]], axis=1)
    down_t = jnp.pad(down_t, ((0, 0), (0, 2 * width)))
    own_w = jnp.where(core == 0, into_w, down_t)
    other_w = jnp.where(core == 0, down_t, into_w)
    own_w, other_w = lax.optimization_barrier((own_w, other_w))
    own_pre = jnp.dot(own, own_w, preferred_element_type=jnp.float32)
    own_pre = lax.optimization_barrier(own_pre)
    other_pre = jnp.dot(other, other_w, preferred_element_type=jnp.float32)
    pre = jnp.where(core == 0, own_pre, other_pre)
    hid = jnp.where(core == 0, other_pre[:, : 2 * width], own_pre[:, : 2 * width])
    gate_pre = pre[:, :width] + jnp.roll(pre[:, width : 2 * width], -1, axis=0)
    up_pre = pre[:, 2 * width : 3 * width] + jnp.roll(pre[:, 3 * width :], -1, axis=0)
    grad_hidden = hid[:, :width] + jnp.roll(hid[:, width:], -1, axis=0)
    gate_sig = jax.nn.sigmoid(gate_pre)
    first = (lax.broadcasted_iota(jnp.int32, (2 * slots, 1), 0) % 2) == 0

    def kept(values):
        return jnp.where(first, values, 0.0).astype(jnp.bfloat16)

    hidden = kept(gate_pre * gate_sig * up_pre)
    grad_up_act = kept(grad_hidden * gate_pre * gate_sig)
    grad_gate_act = kept(grad_hidden * up_pre * gate_sig * (1.0 + gate_pre * (1.0 - gate_sig)))
    acts = jnp.concatenate([grad_gate_act, grad_up_act], axis=1)
    pick = (
        lax.broadcasted_iota(jnp.int32, (slots, 2 * slots), 1)
        == 2 * lax.broadcasted_iota(jnp.int32, (slots, 2 * slots), 0)
    ).astype(jnp.bfloat16)
    acts = jnp.dot(pick, acts, preferred_element_type=jnp.float32).astype(jnp.bfloat16)
    out_w = jnp.concatenate([gate_w, up_w], axis=1).reshape(y_count, 2, width, 2 * width)
    out_own = jnp.where(core == 0, out_w[:, 0], out_w[:, 1]).reshape(half, 2 * width)
    out_other = jnp.where(core == 0, out_w[:, 1], out_w[:, 0]).reshape(half, 2 * width)

    def onto(weights):
        return lax.dot_general(
            acts, weights, (((1,), (1,)), ((), ())), preferred_element_type=jnp.float32
        )

    passed = lax.ppermute(onto(out_other).astype(jnp.bfloat16), "c", [(0, 1), (1, 0)])
    pair_sum = (onto(out_own) + passed.astype(jnp.float32)).astype(jnp.bfloat16)
    parts = pair_sum.reshape(slots, y_count, width).transpose(1, 0, 2)
    swapped = lax.all_to_all(parts, "y", 0, 0, tiled=True)
    summed = sum_parts(swapped).astype(jnp.bfloat16)
    proj_tied, _ = lax.optimization_barrier((proj_near, parts))
    proj_early, _ = lax.optimization_barrier((proj_near, own))
    z_place = lax.axis_index("z")
    blocks = [proj_near] + [None] * 7
    for k in range(1, 8):
        sent_block = proj_near if k in (1, 7) else proj_early if k == 5 else proj_tied
        blocks[k] = lax.ppermute(sent_block, "z", [(i, (i + k) % 8) for i in range(8)])

    def beside(values):
        return jnp.concatenate([values, jnp.roll(values, 1, axis=0)], axis=1)

    grad_in_w = named_dot(
        rows_in, jnp.concatenate([beside(grad_gate_act), beside(grad_up_act)], axis=1)
    )
    grad_gate_w = jnp.concatenate([grad_in_w[:, :width], grad_in_w[:, width : 2 * width]], axis=0)
    grad_up_w = jnp.concatenate(
        [grad_in_w[:, 2 * width : 3 * width], grad_in_w[:, 3 * width :]], axis=0
    )
    grad_out_w = named_dot(beside(hidden), rows_cot)
    grad_down_w = jnp.concatenate([grad_out_w[:width], grad_out_w[width:]], axis=1)

    returned = lax.all_to_all(
        summed.reshape(experts, capacity, -1), SP, split_axis=0, concat_axis=0, tiled=True
    )
    flat_rows = returned.reshape(slots, -1)
    slot_index = lax.broadcasted_iota(jnp.int32, (slots, tokens_here), 0)
    slot_tokens = ((slot_index == slot_a[None, :]) | (slot_index == slot_b[None, :])).astype(
        jnp.bfloat16
    )
    grad_normed = lax.all_gather(
        lax.dot_general(
            slot_tokens, flat_rows, (((0,), (0,)), ((), ())), preferred_element_type=jnp.float32
        ).astype(jnp.bfloat16),
        ("y", "c"),
        axis=1,
        tiled=True,
    )
    query_scale = KEY_CHANNELS ** (-0.5)
    query_rows = query.astype(jnp.float32) * query_scale
    span_log = jnp.cumsum(into_blocks(log_decay), axis=1)
    span_log = jnp.concatenate([span_log[0], span_log[1] + span_log[0, -1:]], axis=0)
    query_cols = jnp.transpose(query_rows * jnp.exp(span_log)).astype(jnp.bfloat16)
    decay_row = jnp.pad(
        jnp.exp(span_log[-1:]), ((0, 7), (0, out_proj.shape[1] - KEY_CHANNELS))
    )
    grad_resid, grad_mixed, near_sent = resid_mixed(
        z_place,
        grad_normed,
        cotangent,
        resid,
        norm_gain,
        blocks,
        query_cols,
        decay_row,
        lax.axis_size("x"),
    )
    share = lax.dot_general(
        grad_resid, mixed, (((0,), (0,)), ((), ())), preferred_element_type=jnp.float32
    ).astype(jnp.bfloat16)
    key_rows = key.astype(jnp.float32)
    value_rows = value.astype(jnp.float32)
    grad_rows = grad_mixed.astype(jnp.float32)
    kept_terms = span_forward(
        query_rows, key_rows, value_rows, grad_rows, log_decay, span_state[0, 0]
    )
    near_filled = lax.all_to_all(near_sent, "x", 0, 0, tiled=True)
    near_states, near_decays = split_decay(near_filled)
    near_sum, near_factor = later_sum(near_states, near_decays, lax.axis_index("x"))
    group_sum, group_factor = later_sum(near_states, near_decays, -1)
    far_filled = to_all(with_decay(group_sum, group_factor), "z")
    far_states, far_decays = split_decay(far_filled)
    z_count, x_count = lax.axis_size("z"), lax.axis_size("x")
    share_rows = model_width // sp_count
    share_x = share.reshape(z_count, x_count, share_rows, -1).transpose(1, 0, 2, 3)
    place = lax.axis_index("x")

    def for_place(k):
        at = jnp.bitwise_and(place + k, x_count - 1).astype(jnp.uint32)
        return lax.dynamic_index_in_dim(share_x, at, 0, keepdims=False)

    share_sum = for_place(0).astype(jnp.float32)
    for k in range(1, 4):
        passed = lax.ppermute(
            for_place(k), "x", [(i, (i + k) % 4) for i in range(4)]
        )
        share_sum = share_sum + passed.astype(jnp.float32)
    share_z = share_sum.astype(jnp.bfloat16)
    share_z = lax.all_to_all(share_z, "z", 0, 0, tiled=True)
    grad_out_proj = sum_parts(share_z)
    far_sum, _ = later_sum(far_states, far_decays, lax.axis_index("z"))
    exit_cot = near_sum + near_factor[:, None] * far_sum
    grad_query, grad_key, grad_value, grad_log_decay = span_backward(
        query_rows, key_rows, value_rows, grad_rows, kept_terms, exit_cot
    )
    grad_query = (grad_query * query_scale).astype(jnp.bfloat16)
    grad_key = grad_key.astype(jnp.bfloat16)
    grad_value = grad_value.astype(jnp.bfloat16)
    return (
        grad_gate_w[None],
        grad_up_w[None],
        grad_down_w[None],
        grad_out_proj,
        grad_query,
        grad_key,
        grad_value,
        grad_log_decay,
    )


def solution(mesh):
    finer = Mesh(mesh.devices.reshape(8, 4, 8, 2), ("z", "x", "y", "c"))
    in_specs = (
        P(SP, None),
        P(),
        P(SP, None),
        P(SP, None),
        P(SP, None),
        P(SP, None, TP),
        P(SP, None, TP),
        P(SP, TP, None),
        P(SP, TP),
        P(SP, TP),
        P(SP, TP),
        P(SP, TP),
        P(SP, TP),
        P(SP, TP),
        P(SP, TP, None, None),
    )
    out_specs = (
        P(SP, None, TP),
        P(SP, None, TP),
        P(SP, TP, None),
        P(SP, TP),
        P(SP, TP),
        P(SP, TP),
        P(SP, TP),
        P(SP, TP),
    )
    return jax.shard_map(
        on_device_body, mesh=finer, in_specs=in_specs, out_specs=out_specs, check_vma=False
    )
```

```python
import jax
import jax.numpy as jnp
from jax import lax
from jax.experimental import pallas as pl
from jax.experimental.pallas import tpu as pltpu
from jax.sharding import Mesh
from jax.sharding import PartitionSpec as P


KEY_CHANNELS = 128
CAPACITY = 12
BLOCK = 64
SP = ("z", "x")
TP = ("y", "c")


epsilon = 1e-06


def sum_parts(tiles):
    return jnp.sum(tiles.astype(jnp.float32), axis=0)


def later_sum(states, decays, place):
    count = states.shape[0]
    total = jnp.zeros(states.shape[1:], jnp.float32)
    factor = jnp.ones(decays.shape[1:], jnp.float32)
    for k in range(count):
        later = k > place
        total = total + jnp.where(later, factor, 0.0)[:, None] * states[k].astype(jnp.float32)
        factor = jnp.where(later, factor * decays[k], factor)
    return total, factor


def named_dot(left, right):
    return lax.dot_general(
        left, right, (((0,), (0,)), ((), ())), preferred_element_type=jnp.float32
    ).astype(jnp.bfloat16)


def to_all(array, axis):
    count = lax.axis_size(axis)
    copies = jnp.broadcast_to(array[None], (count, *array.shape))
    return lax.all_to_all(copies, axis, 0, 0, tiled=True)


def into_blocks(values):
    return values.reshape(values.shape[0] // BLOCK, BLOCK, values.shape[1])


def span_forward(query_rows, key_rows, value_rows, grad_rows, decay_rows, entry_state):
    query_blk = into_blocks(query_rows)
    key_blk = into_blocks(key_rows)
    value_blk = into_blocks(value_rows)
    grad_blk = into_blocks(grad_rows)
    cumlog = jnp.cumsum(into_blocks(decay_rows), axis=1)
    block_total = cumlog[:, -1, :]
    to_end = jnp.exp(block_total[:, None, :] - cumlog)
    inner_part = jnp.einsum("nsd,nsj->ndj", key_blk * to_end, value_blk)

    def forward_step(carry_state, step_item):
        piece_part, block_sum = step_item
        return (jnp.exp(block_sum)[:, None] * carry_state + piece_part, carry_state)

    end_state, starts = lax.scan(
        forward_step, entry_state, (inner_part, block_total), unroll=True
    )
    second_part = jnp.einsum("td,tj->dj", query_blk[1] * jnp.exp(cumlog[1]), grad_blk[1])
    after_cot = jnp.stack([second_part, jnp.zeros_like(second_part)])
    span_total = jnp.sum(block_total, axis=0)
    later_log = span_total[None, :] - jnp.cumsum(block_total, axis=0)
    return (cumlog, starts, after_cot, later_log, end_state)


def span_backward(query_rows, key_rows, value_rows, grad_rows, kept_terms, exit_cot):
    cumlog, starts, after_cot, later_log, end_state = kept_terms
    query_blk = into_blocks(query_rows)
    key_blk = into_blocks(key_rows)
    value_blk = into_blocks(value_rows)
    grad_blk = into_blocks(grad_rows)
    exit_cots = after_cot + jnp.exp(later_log)[:, :, None] * exit_cot
    causal = jnp.arange(BLOCK)[:, None] >= jnp.arange(BLOCK)[None, :]
    decays = jnp.exp(
        jnp.where(causal[None, :, :, None], cumlog[:, :, None, :] - cumlog[:, None, :, :], -jnp.inf)
    )
    scores = jnp.einsum("ntd,nsd,ntsd->nts", query_blk, key_blk, decays)
    grad_scores = jnp.einsum("ntj,nsj->nts", grad_blk, value_blk)
    grad_query = jnp.exp(cumlog) * jnp.einsum("ntj,ndj->ntd", grad_blk, starts)
    grad_query = grad_query + jnp.einsum("nts,nsd,ntsd->ntd", grad_scores, key_blk, decays)
    to_end = jnp.exp(cumlog[:, -1:, :] - cumlog)
    grad_key = jnp.einsum("nts,ntd,ntsd->nsd", grad_scores, query_blk, decays)
    grad_key = grad_key + to_end * jnp.einsum("nsj,ndj->nsd", value_blk, exit_cots)
    grad_value = jnp.einsum("nts,ntj->nsj", scores, grad_blk)
    grad_value = grad_value + jnp.einsum("nsd,ndj->nsj", key_blk * to_end, exit_cots)
    length = query_rows.shape[0]
    key_width = query_rows.shape[1]
    per_position = (query_blk * grad_query - key_blk * grad_key).reshape(length, key_width)
    grad_log = (
        jnp.flip(jnp.cumsum(jnp.flip(per_position, 0), 0), 0)
        + jnp.sum(end_state * exit_cot, axis=1)[None, :]
    )
    return (
        grad_query.reshape(length, key_width),
        grad_key.reshape(length, key_width),
        grad_value.reshape(length, value_rows.shape[1]),
        grad_log,
    )


def dispatch_rows_kernel(core_ref, ids_ref, weight_ref, resid_ref, cot_ref, gain_ref, sent_ref, slot_ref, rows_ref):
    tokens, model_width = resid_ref.shape
    half = model_width // 2
    experts = sent_ref.shape[0] // (2 * CAPACITY)

    square = (tokens, tokens)
    row_at = lax.broadcasted_iota(jnp.int32, square, 0)
    col_at = lax.broadcasted_iota(jnp.int32, square, 1)
    along = [ids_ref[k : k + 1, :].astype(jnp.float32) for k in range(2)]

    @pl.when(core_ref[0] == 0)
    def _():
        for at in range(0, tokens, 32):
            r = resid_ref[at : at + 32, :].astype(jnp.float32)
            inverse_rms = lax.rsqrt(jnp.mean(r * r, axis=1, keepdims=True) + epsilon)
            normed = (r * inverse_rms * gain_ref[...]).astype(jnp.bfloat16)
            for k in range(2):
                for h in range(2):
                    low = (2 * k + h) * tokens + at
                    rows_ref[low : low + 32, :] = normed[:, h * half : (h + 1) * half]

    @pl.when(core_ref[0] != 0)
    def _():
        weights = []
        for k in range(2):
            spread = jnp.broadcast_to(weight_ref[k : k + 1, :], square)
            weights.append(
                jnp.sum(jnp.where(row_at == col_at, spread, 0.0), axis=1, keepdims=True)
            )
        for at in range(0, tokens, 32):
            c = cot_ref[at : at + 32, :].astype(jnp.float32)
            for k in range(2):
                sent = (c * weights[k][at : at + 32, :]).astype(jnp.bfloat16)
                for h in range(2):
                    low = (2 * k + h) * tokens + at
                    rows_ref[low : low + 32, :] = sent[:, h * half : (h + 1) * half]

    expert_at = lax.broadcasted_iota(jnp.int32, (experts, tokens), 0).astype(jnp.float32)
    named = [(expert_at == a).astype(jnp.float32) for a in along]
    earlier = (row_at < col_at).astype(jnp.bfloat16)
    before = jnp.dot(
        (named[0] + named[1]).astype(jnp.bfloat16), earlier, preferred_element_type=jnp.float32
    )
    slots = [
        (a * CAPACITY + jnp.sum(n * before, axis=0, keepdims=True)).astype(jnp.int32)
        for a, n in zip(along, named)
    ]
    slot_ref[...] = jnp.concatenate(slots + [jnp.zeros((6, tokens), jnp.int32)], axis=0)
    step = 256
    for at in range(0, sent_ref.shape[0], step):
        packed = lax.broadcasted_iota(jnp.int32, (step, tokens), 0) + at
        hits = [
            jnp.where(packed == 2 * slot + h, 1.0, 0.0).astype(jnp.bfloat16)
            for slot in slots
            for h in range(2)
        ]
        sent_ref[at : at + step, :] = jnp.dot(
            jnp.concatenate(hits, axis=1), rows_ref[...], preferred_element_type=jnp.float32
        ).astype(jnp.bfloat16)


def dispatch_rows(core, ids, weight, resid, cotangent, gain, experts):
    tokens, model_width = resid.shape
    half = model_width // 2
    vmem = pl.BlockSpec(memory_space=pltpu.VMEM)
    return pl.pallas_call(
        dispatch_rows_kernel,
        out_shape=(
            jax.ShapeDtypeStruct((2 * experts * CAPACITY, half), jnp.bfloat16),
            jax.ShapeDtypeStruct((8, tokens), jnp.int32),
        ),
        in_specs=[pl.BlockSpec(memory_space=pltpu.SMEM)] + [vmem] * 5,
        out_specs=(vmem, vmem),
        scratch_shapes=[pltpu.VMEM((4 * tokens, half), jnp.bfloat16)],
        name="dispatch_rows",
    )(core.astype(jnp.int32).reshape(1), ids.T, weight.T, resid, cotangent, gain.reshape(1, -1))


def resid_mixed_kernel(
    place_ref, normed_ref, cot_ref, resid_ref, gain_ref, query_ref, *refs
):
    blocks, (out_ref, mixed_ref, near_ref) = refs[:8], refs[8:]
    tokens = resid_ref.shape[0]
    for at in range(0, tokens, 32):
        rows = slice(at, at + 32)
        r = resid_ref[rows, :].astype(jnp.float32)
        inverse_rms = lax.rsqrt(jnp.mean(r * r, axis=1, keepdims=True) + epsilon)
        unit = r * inverse_rms
        scaled = normed_ref[rows, :].astype(jnp.float32) * gain_ref[...]
        mean = jnp.mean(scaled * unit, axis=1, keepdims=True)
        grad = cot_ref[rows, :].astype(jnp.float32) + inverse_rms * (scaled - unit * mean)
        out_ref[rows, :] = grad.astype(jnp.bfloat16)
    depth = blocks[0].shape[0]
    total = jnp.zeros(mixed_ref.shape, jnp.float32)
    for k in range(8):
        at = pl.multiple_of(jnp.bitwise_and(place_ref[0] + (8 - k), 7) * depth, depth)
        total = total + jnp.dot(
            out_ref[:, pl.ds(at, depth)], blocks[k][...], preferred_element_type=jnp.float32
        )
    mixed = total.astype(jnp.bfloat16)
    mixed_ref[...] = mixed
    state = jnp.dot(query_ref[...], mixed, preferred_element_type=jnp.float32)
    for k in range(near_ref.shape[0]):
        near_ref[k] = state.astype(jnp.bfloat16)


def resid_mixed(place, grad_normed, cotangent, resid, gain, blocks, query_cols, copies):
    vmem = pl.BlockSpec(memory_space=pltpu.VMEM)
    return pl.pallas_call(
        resid_mixed_kernel,
        out_shape=(
            jax.ShapeDtypeStruct(resid.shape, jnp.bfloat16),
            jax.ShapeDtypeStruct((resid.shape[0], blocks[0].shape[1]), jnp.bfloat16),
            jax.ShapeDtypeStruct(
                (copies, query_cols.shape[0], blocks[0].shape[1]), jnp.bfloat16
            ),
        ),
        in_specs=[pl.BlockSpec(memory_space=pltpu.SMEM)] + [vmem] * 13,
        out_specs=(vmem, vmem, vmem),
        name="resid_mixed",
    )(
        place.astype(jnp.int32).reshape(1),
        grad_normed,
        cotangent,
        resid,
        gain.reshape(1, -1),
        query_cols,
        *blocks,
    )


def on_device_body(
    resid,
    norm_gain,
    cotangent,
    route_ids,
    route_weight,
    expert_gate,
    expert_up,
    expert_down,
    out_proj,
    mixed,
    query,
    key,
    value,
    log_decay,
    span_state,
):
    tokens_here = resid.shape[0]
    model_width = resid.shape[1]
    half = model_width // 2
    sp_count = lax.axis_size(SP)
    y_count = lax.axis_size("y")
    experts = sp_count * expert_gate.shape[0]
    capacity = CAPACITY
    slots = experts * capacity
    core = lax.axis_index("c")
    sent, slot_rows = dispatch_rows(
        core, route_ids, route_weight, resid, cotangent, norm_gain, experts
    )
    slot_a, slot_b = slot_rows[0], slot_rows[1]
    sent = sent.reshape(sp_count, 2 * capacity, half)
    gate_w, up_w, down_w = expert_gate[0], expert_up[0], expert_down[0]
    width = gate_w.shape[1]
    own = lax.all_to_all(sent, SP, 0, 0, tiled=True).reshape(2 * slots, half)
    proj_near, _ = lax.optimization_barrier((out_proj, sent))
    proj_near = lax.all_gather(proj_near, "x", axis=0, tiled=True)
    other = lax.ppermute(own, "c", [(0, 1), (1, 0)])
    rows_in = jnp.where(core == 0, own, other)
    rows_cot = jnp.where(core == 0, other, own)

    into_w = jnp.concatenate([gate_w[:half], gate_w[half:], up_w[:half], up_w[half:]], axis=1)
    down_t = jnp.transpose(down_w)
    down_t = jnp.concatenate([down_t[:half], down_t[half:]], axis=1)
    down_t = jnp.pad(down_t, ((0, 0), (0, 2 * width)))
    own_w = jnp.where(core == 0, into_w, down_t)
    other_w = jnp.where(core == 0, down_t, into_w)
    own_w, other_w = lax.optimization_barrier((own_w, other_w))
    own_pre = jnp.dot(own, own_w, preferred_element_type=jnp.float32)
    own_pre = lax.optimization_barrier(own_pre)
    other_pre = jnp.dot(other, other_w, preferred_element_type=jnp.float32)
    pre = jnp.where(core == 0, own_pre, other_pre)
    hid = jnp.where(core == 0, other_pre[:, : 2 * width], own_pre[:, : 2 * width])
    gate_pre = pre[:, :width] + jnp.roll(pre[:, width : 2 * width], -1, axis=0)
    up_pre = pre[:, 2 * width : 3 * width] + jnp.roll(pre[:, 3 * width :], -1, axis=0)
    grad_hidden = hid[:, :width] + jnp.roll(hid[:, width:], -1, axis=0)
    gate_sig = jax.nn.sigmoid(gate_pre)
    first = (lax.broadcasted_iota(jnp.int32, (2 * slots, 1), 0) % 2) == 0

    def kept(values):
        return jnp.where(first, values, 0.0).astype(jnp.bfloat16)

    hidden = kept(gate_pre * gate_sig * up_pre)
    grad_up_act = kept(grad_hidden * gate_pre * gate_sig)
    grad_gate_act = kept(grad_hidden * up_pre * gate_sig * (1.0 + gate_pre * (1.0 - gate_sig)))
    acts = jnp.concatenate([grad_gate_act, grad_up_act], axis=1)
    pick = (
        lax.broadcasted_iota(jnp.int32, (slots, 2 * slots), 1)
        == 2 * lax.broadcasted_iota(jnp.int32, (slots, 2 * slots), 0)
    ).astype(jnp.bfloat16)
    acts = jnp.dot(pick, acts, preferred_element_type=jnp.float32).astype(jnp.bfloat16)
    out_w = jnp.concatenate([gate_w, up_w], axis=1).reshape(y_count, 2, width, 2 * width)
    out_own = jnp.where(core == 0, out_w[:, 0], out_w[:, 1]).reshape(half, 2 * width)
    out_other = jnp.where(core == 0, out_w[:, 1], out_w[:, 0]).reshape(half, 2 * width)

    def onto(weights):
        return lax.dot_general(
            acts, weights, (((1,), (1,)), ((), ())), preferred_element_type=jnp.float32
        )

    passed = lax.ppermute(onto(out_other).astype(jnp.bfloat16), "c", [(0, 1), (1, 0)])
    pair_sum = (onto(out_own) + passed.astype(jnp.float32)).astype(jnp.bfloat16)
    parts = pair_sum.reshape(slots, y_count, width).transpose(1, 0, 2)
    swapped = lax.all_to_all(parts, "y", 0, 0, tiled=True)
    summed = sum_parts(swapped).astype(jnp.bfloat16)
    proj_tied, _ = lax.optimization_barrier((proj_near, parts))
    z_place = lax.axis_index("z")
    blocks = [proj_near] + [None] * 7
    for k in range(1, 8):
        sent_block = proj_near if k in (1, 7) else proj_tied
        blocks[k] = lax.ppermute(sent_block, "z", [(i, (i + k) % 8) for i in range(8)])

    def beside(values):
        return jnp.concatenate([values, jnp.roll(values, 1, axis=0)], axis=1)

    grad_in_w = named_dot(
        rows_in, jnp.concatenate([beside(grad_gate_act), beside(grad_up_act)], axis=1)
    )
    grad_gate_w = jnp.concatenate([grad_in_w[:, :width], grad_in_w[:, width : 2 * width]], axis=0)
    grad_up_w = jnp.concatenate(
        [grad_in_w[:, 2 * width : 3 * width], grad_in_w[:, 3 * width :]], axis=0
    )
    grad_out_w = named_dot(beside(hidden), rows_cot)
    grad_down_w = jnp.concatenate([grad_out_w[:width], grad_out_w[width:]], axis=1)

    query_scale = KEY_CHANNELS ** (-0.5)
    query_rows = query.astype(jnp.float32) * query_scale
    span_log = jnp.cumsum(into_blocks(log_decay), axis=1)
    span_log = jnp.concatenate([span_log[0], span_log[1] + span_log[0, -1:]], axis=0)
    query_cols = jnp.transpose(query_rows * jnp.exp(span_log)).astype(jnp.bfloat16)
    own_decay = jnp.exp(span_log[-1:]).astype(jnp.bfloat16)
    chunks = jnp.concatenate(
        [
            summed.reshape(experts, capacity, -1),
            jnp.broadcast_to(own_decay[None], (experts, 4, KEY_CHANNELS)),
        ],
        axis=1,
    )
    returned = lax.all_to_all(chunks, SP, split_axis=0, concat_axis=0, tiled=True)
    flat_rows = returned[:, :capacity].reshape(slots, -1)
    decays = returned[:, capacity].astype(jnp.float32)
    decays = decays.reshape(lax.axis_size("z"), lax.axis_size("x"), KEY_CHANNELS)
    near_decays = lax.dynamic_index_in_dim(
        decays, lax.axis_index("z").astype(jnp.uint32), 0, keepdims=False
    )
    far_decays = jnp.prod(decays, axis=1)
    slot_index = lax.broadcasted_iota(jnp.int32, (slots, tokens_here), 0)
    slot_tokens = ((slot_index == slot_a[None, :]) | (slot_index == slot_b[None, :])).astype(
        jnp.bfloat16
    )
    grad_normed = lax.all_gather(
        lax.dot_general(
            slot_tokens, flat_rows, (((0,), (0,)), ((), ())), preferred_element_type=jnp.float32
        ).astype(jnp.bfloat16),
        ("y", "c"),
        axis=1,
        tiled=True,
    )
    grad_resid, grad_mixed, near_sent = resid_mixed(
        z_place,
        grad_normed,
        cotangent,
        resid,
        norm_gain,
        blocks,
        query_cols,
        lax.axis_size("x"),
    )
    share = lax.dot_general(
        grad_resid, mixed, (((0,), (0,)), ((), ())), preferred_element_type=jnp.float32
    ).astype(jnp.bfloat16)
    key_rows = key.astype(jnp.float32)
    value_rows = value.astype(jnp.float32)
    grad_rows = grad_mixed.astype(jnp.float32)
    kept_terms = span_forward(
        query_rows, key_rows, value_rows, grad_rows, log_decay, span_state[0, 0]
    )
    near_filled = lax.all_to_all(near_sent, "x", 0, 0, tiled=True)
    near_sum, near_factor = later_sum(near_filled, near_decays, lax.axis_index("x"))
    group_sum, _ = later_sum(near_filled, near_decays, -1)
    far_filled = to_all(group_sum.astype(jnp.bfloat16), "z")
    z_count, x_count = lax.axis_size("z"), lax.axis_size("x")
    share_rows = model_width // sp_count
    share_x = share.reshape(z_count, x_count, share_rows, -1).transpose(1, 0, 2, 3)
    place = lax.axis_index("x")

    def for_place(k):
        at = jnp.bitwise_and(place + k, x_count - 1).astype(jnp.uint32)
        return lax.dynamic_index_in_dim(share_x, at, 0, keepdims=False)

    share_sum = for_place(0).astype(jnp.float32)
    for k in range(1, 4):
        passed = lax.ppermute(
            for_place(k), "x", [(i, (i + k) % 4) for i in range(4)]
        )
        share_sum = share_sum + passed.astype(jnp.float32)
    share_z = share_sum.astype(jnp.bfloat16)
    share_z = lax.all_to_all(share_z, "z", 0, 0, tiled=True)
    grad_out_proj = sum_parts(share_z)
    far_sum, _ = later_sum(far_filled, far_decays, lax.axis_index("z"))
    exit_cot = near_sum + near_factor[:, None] * far_sum
    grad_query, grad_key, grad_value, grad_log_decay = span_backward(
        query_rows, key_rows, value_rows, grad_rows, kept_terms, exit_cot
    )
    grad_query = (grad_query * query_scale).astype(jnp.bfloat16)
    grad_key = grad_key.astype(jnp.bfloat16)
    grad_value = grad_value.astype(jnp.bfloat16)
    return (
        grad_gate_w[None],
        grad_up_w[None],
        grad_down_w[None],
        grad_out_proj,
        grad_query,
        grad_key,
        grad_value,
        grad_log_decay,
    )


def solution(mesh):
    finer = Mesh(mesh.devices.reshape(8, 4, 8, 2), ("z", "x", "y", "c"))
    in_specs = (
        P(SP, None),
        P(),
        P(SP, None),
        P(SP, None),
        P(SP, None),
        P(SP, None, TP),
        P(SP, None, TP),
        P(SP, TP, None),
        P(SP, TP),
        P(SP, TP),
        P(SP, TP),
        P(SP, TP),
        P(SP, TP),
        P(SP, TP),
        P(SP, TP, None, None),
    )
    out_specs = (
        P(SP, None, TP),
        P(SP, None, TP),
        P(SP, TP, None),
        P(SP, TP),
        P(SP, TP),
        P(SP, TP),
        P(SP, TP),
        P(SP, TP),
    )
    return jax.shard_map(
        on_device_body, mesh=finer, in_specs=in_specs, out_specs=out_specs, check_vma=False
    )
```
